32 devices in a mesh: ep: 16 (over z, x, core), tp: 2 (over y).
Axes of the slice: x: 2, y: 2, z: 4, core: 2. Of those that a mesh axis runs over, the one named last changes fastest.
Arguments:
- residual_in: bfloat16 [240, 1536], P('ep'), may hold values from -6 to 6
- rec_state: bfloat16 [240, 12, 128, 128], P('ep', 'tp'), may hold values from -6 to 6
- mix_gain: float32 [1536], replicated, may hold values from 0.1 to 1.9
- w_query: bfloat16 [1536, 1536], P('tp', 'ep'), may hold values from -0.15625 to 0.15625
- w_forget: bfloat16 [1536, 1536], P('tp', 'ep'), may hold values from -0.15625 to 0.15625
- w_input: bfloat16 [1536, 1536], P('tp', 'ep'), may hold values from -0.15625 to 0.15625
- w_gate: bfloat16 [1536, 1536], P('tp', 'ep'), may hold values from -0.15625 to 0.15625
- lower_bound: float32 [1536], P('tp'), may hold values from 0 to 0.9
- head_gain: float32 [128], replicated, may hold values from 0.1 to 1.9
- w_out: bfloat16 [1536, 1536], P('tp', 'ep'), may hold values from -0.15625 to 0.15625
- ffn_gain: float32 [1536], replicated, may hold values from 0.1 to 1.9
- route_ids: int32 [240, 6], P('ep'), may hold values from 0 to 15, all different within a row; in each aligned block of 15 rows (0 to 14, 15 to 29, ...) at most 6 rows name the same one
- route_weight: float32 [240, 6], P('ep'), may hold values from 0.2 to 1
- expert_gate: bfloat16 [16, 1536, 512], P('ep', None, 'tp'), may hold values from -0.15625 to 0.15625
- expert_up: bfloat16 [16, 1536, 512], P('ep', None, 'tp'), may hold values from -0.15625 to 0.15625
- expert_down: bfloat16 [16, 512, 1536], P('ep', 'tp'), may hold values from -0.25 to 0.25
Outputs:
- layer_out: bfloat16 [240, 1536], P('ep', 'tp')
- new_state: bfloat16 [240, 12, 128, 128], P('ep', 'tp')
The draws below stay inside these ranges and needn't reach their ends.
Inputs may be any that keep to these rules, and one draw needn't show every extreme that they name: `route_ids`: each row names 6 different experts. Among the rows of one device no expert is named more than 6 times, and in every draw some device names some expert exactly 6 times.
All inputs are finite; a program needn't handle non-finite values.
Results may differ from the reference program's by a relative error of at most 0.016.
Values may be sent and summed in bfloat16 or wider, within the bound.
No kernel may reach another device: no remote copies, remote signals or barrier semaphores. Data moves between devices by JAX's collectives and lax.ppermute only.
A program may use at most 64 MiB of HBM per device.

```python
import math
import jax
import jax.numpy as jnp
import numpy as np
from jax import lax

D = 1536
HEADS = 12
FF = 512
TOPK = 6
SEQ_DEV = 15
HEAD = 128
TOKENS = 240
EXPERTS = 16
CAP = 6
N_EP = 16


def level_of(rng, dims, split, least, largest):
    level, own = 1.0, jax.random.fold_in(rng, 6)
    for position, shards_of in split:
        draws = jnp.exp(jax.random.uniform(jax.random.fold_in(own, position), (shards_of,), jnp.float32, least / len(split), largest / len(split)))
        level = level * jnp.repeat(draws, dims[position] // shards_of).reshape([-1 if axis == position else 1 for axis in range(len(dims))])
    return level


def shared_out(rng, own, number, rows, amount, top, bound, slope):
    ranking = jax.random.permutation(rng, amount)
    crowded, usual = shares(amount, rows * top, bound, slope, True), shares(amount, rows * top, bound, slope, False)
    places = jnp.arange(amount)

    def named(tallies, offset_by):
        used = int((tallies > 0).sum())
        fixed = max(1, used // 4)
        shifted = fixed + (places - fixed + offset_by * (used - fixed)) % max(1, amount - fixed)
        return jnp.zeros((amount,), jnp.int32).at[ranking[jnp.where(places < fixed, places, shifted)]].set(jnp.asarray(tallies, jnp.int32))

    tallies = jnp.where(number % 4 == 0, named(crowded, number // 4), named(usual, number - number // 4 - 1))
    mixed = jax.random.permutation(jax.random.fold_in(own, 3), amount)
    giver, sink = mixed[0:amount // 2 * 2:2], mixed[1:amount // 2 * 2:2]
    slack = jnp.minimum(tallies[giver] - 1, bound - tallies[sink]) // 2
    slack = jnp.where((giver == ranking[0]) | (sink == ranking[0]) | (tallies[sink] == 0), 0, jnp.maximum(slack, 0))
    shifted = jax.random.randint(jax.random.fold_in(own, 4), (amount // 2,), 0, 1 << 20) % (slack + 1)
    tallies = tallies.at[giver].add(-shifted).at[sink].add(shifted)
    members = jnp.searchsorted(jnp.cumsum(tallies), jnp.arange(rows * top), side="right").astype(jnp.int32)
    listing = members.reshape(top, rows).T
    listing = listing[jax.random.permutation(jax.random.fold_in(own, 1), rows)]
    offset_by = jax.random.randint(jax.random.fold_in(own, 2), (rows, 1), 0, top)
    return jnp.take_along_axis(listing, (jnp.arange(top)[None, :] + offset_by) % top, axis=1)


def shares(count, total, reach, lean, full):
    loads = [(1 << 20) // math.isqrt(rank ** lean) + 1 for rank in range(1, count + 1)]
    largest = reach if full else min(reach, max(-(-total // count), total * loads[0] // sum(loads)))
    least = 1 if total - largest >= count - 1 else 0
    given, rest = [largest] + [least] * (count - 1), total - largest - least * (count - 1)
    while rest > 0:
        candidates = [i for i in range(1, count) if given[i] < largest] or [i for i in range(1, count) if given[i] < reach]
        mass, remaining = sum([loads[i] for i in candidates]), rest
        for i in candidates:
            extra = min(reach - given[i], max(1, remaining * loads[i] // mass), rest)
            given[i] = given[i] + extra
            rest = rest - extra
    return np.array(given)


def bell_draw(key, dims, width, reach, pieces=(), kind=jnp.bfloat16):
    result = jax.random.normal(key, dims, jnp.float32) * width
    if len(pieces) > 0:
        result = level_of(key, dims, pieces, -0.22, 0.18) * result
    return jnp.clip(result, min=-reach, max=reach).astype(kind)


def setup_inputs(seed: int = 0) -> dict:
    keys = jax.random.split(jax.random.key(seed), 17)
    residual_in = bell_draw(keys[0], (TOKENS, D), 1.0, 6.0, ((0, 16),))
    rec_state = bell_draw(keys[1], (TOKENS, HEADS, HEAD, HEAD), 1.0, 6.0, ((0, 16), (1, 2)))
    mix_gain = jnp.clip(1.0 + 0.18 * jax.random.normal(keys[2], (D,), jnp.float32), 0.1, 1.9)
    w_query = bell_draw(keys[3], (D, D), D ** -0.5, 0.15625, ((0, 2), (1, 16)))
    w_forget = bell_draw(keys[4], (D, D), D ** -0.5, 0.15625, ((0, 2), (1, 16)))
    w_input = bell_draw(keys[5], (D, D), D ** -0.5, 0.15625, ((0, 2), (1, 16)))
    w_gate = bell_draw(keys[6], (D, D), D ** -0.5, 0.15625, ((0, 2), (1, 16)))
    lower_bound = jnp.clip(0.9 * jax.random.uniform(keys[7], (D,), jnp.float32) ** level_of(keys[7], (D,), ((0, 2),), -0.2, 0.2), 0.0, 0.9)
    head_gain = jnp.clip(1.0 + 0.18 * jax.random.normal(keys[8], (HEAD,), jnp.float32), 0.1, 1.9)
    w_out = bell_draw(keys[9], (D, D), D ** -0.5, 0.15625, ((0, 2), (1, 16)))
    ffn_gain = jnp.clip(1.0 + 0.18 * jax.random.normal(keys[10], (D,), jnp.float32), 0.1, 1.9)
    route_ids_keys = jax.random.split(jax.random.fold_in(keys[11], 1), TOKENS // SEQ_DEV)
    route_ids_turns = jax.random.permutation(jax.random.fold_in(keys[11], 3), TOKENS // SEQ_DEV)
    route_ids = jax.vmap(lambda own, number: shared_out(jax.random.fold_in(keys[11], 2), own, number, SEQ_DEV, EXPERTS, TOPK, CAP, 2))(route_ids_keys, route_ids_turns).reshape((TOKENS, TOPK))
    route_weight = jnp.clip(jnp.exp(math.log(1.0) - 1.609438 * jax.random.uniform(keys[12], (TOKENS, TOPK), jnp.float32) ** level_of(keys[12], (TOKENS, TOPK), ((0, 16),), -0.2, 0.2)), 0.2, 1.0)
    expert_gate = bell_draw(keys[13], (EXPERTS, D, FF), D ** -0.5, 0.15625, ((0, 16), (2, 2)))
    expert_up = bell_draw(keys[14], (EXPERTS, D, FF), D ** -0.5, 0.15625, ((0, 16), (2, 2)))
    expert_down = bell_draw(keys[15], (EXPERTS, FF, D), FF ** -0.5, 0.25, ((0, 16), (1, 2)))
    return dict(residual_in=residual_in, rec_state=rec_state, mix_gain=mix_gain, w_query=w_query, w_forget=w_forget, w_input=w_input, w_gate=w_gate, lower_bound=lower_bound, head_gain=head_gain, w_out=w_out, ffn_gain=ffn_gain, route_ids=route_ids, route_weight=route_weight, expert_gate=expert_gate, expert_up=expert_up, expert_down=expert_down)


rms_eps = 1e-06

def rms_scale(values, gain):
    return values * lax.rsqrt(lax.optimization_barrier(jnp.mean(values * values, axis=-1, keepdims=True)) + rms_eps) * gain

def rounded(values):
    return lax.optimization_barrier(values.astype(jnp.bfloat16)).astype(jnp.float32)

def recurrence(lower_bound, head_gain, state_block, query_raw, forget_raw, input_raw, gate_raw):
    seq_count = state_block.shape[0]
    heads_local = state_block.shape[1]
    head_size = state_block.shape[2]
    head_shape = (seq_count, heads_local, head_size)
    forget = lower_bound + (1.0 - lower_bound) * jax.nn.sigmoid(forget_raw)
    query_act = jax.nn.silu(query_raw).reshape(head_shape)
    key_act = (1.0 - forget).reshape(head_shape)
    forget_heads = forget.reshape(head_shape)
    value_act = input_raw.reshape(head_shape)
    state_next = forget_heads[:, :, :, None] * state_block.astype(jnp.float32) + key_act[:, :, :, None] * value_act[:, :, None, :]
    readout = jnp.einsum('shk,shkv->shv', query_act, state_next, precision=lax.Precision.HIGHEST)
    gate_heads = jax.nn.silu(gate_raw).reshape(head_shape)
    heads_out = rms_scale(readout, head_gain) * gate_heads
    return (state_next.astype(jnp.bfloat16), heads_out.reshape(seq_count, heads_local * head_size).astype(jnp.bfloat16))

def reference(residual_in, rec_state, mix_gain, w_query, w_forget, w_input, w_gate, lower_bound, head_gain, w_out, ffn_gain, route_ids, route_weight, expert_gate, expert_up, expert_down):
    residual = residual_in.astype(jnp.float32)
    normed = rms_scale(residual, mix_gain).astype(jnp.bfloat16)
    projected = [rounded(jnp.dot(normed, weight, preferred_element_type=jnp.float32)) for weight in (w_query, w_forget, w_input, w_gate)]

    def to_blocks(values):
        return values.reshape((N_EP, SEQ_DEV) + values.shape[1:])

    def per_block(blocks):
        return recurrence(lower_bound, head_gain, blocks[0], blocks[1], blocks[2], blocks[3], blocks[4])
    state_next, heads_out = lax.map(per_block, (to_blocks(rec_state), to_blocks(projected[0]), to_blocks(projected[1]), to_blocks(projected[2]), to_blocks(projected[3])))
    new_state = state_next.reshape(rec_state.shape)
    heads_out = heads_out.reshape(TOKENS, D)
    mixed = jnp.dot(heads_out, w_out, preferred_element_type=jnp.float32)
    after_mix = rounded(residual + mixed)
    normed_ffn = rms_scale(after_mix, ffn_gain).astype(jnp.bfloat16)

    def one_slot(slot_args):
        row_values = slot_args[0]
        expert_id = slot_args[1]
        gate_part = jnp.dot(row_values, expert_gate[expert_id], preferred_element_type=jnp.float32)
        up_part = jnp.dot(row_values, expert_up[expert_id], preferred_element_type=jnp.float32)
        hidden = (jax.nn.silu(gate_part) * up_part).astype(jnp.bfloat16)
        return jnp.dot(hidden, expert_down[expert_id], preferred_element_type=jnp.float32).astype(jnp.bfloat16)
    slot_rows = jnp.repeat(normed_ffn, TOPK, axis=0)
    expert_rows = lax.map(one_slot, (slot_rows, route_ids.reshape(-1).astype(jnp.int32)))
    expert_sum = lax.optimization_barrier(jnp.sum(route_weight[:, :, None] * expert_rows.reshape(TOKENS, TOPK, D).astype(jnp.float32), axis=1))
    layer_out = (after_mix + expert_sum).astype(jnp.bfloat16)
    return (layer_out, new_state)
```

```python
import functools

import jax
import jax.numpy as jnp
from jax import lax
from jax.experimental import pallas as pl
from jax.experimental.pallas import tpu as pltpu
from jax.sharding import Mesh, PartitionSpec as P

rms_eps = 1e-06
bf16, f32 = jnp.bfloat16, jnp.float32


def dot(a, b):
    return jnp.dot(a, b, preferred_element_type=f32)


def rms_scale(values, gain):
    return values * lax.rsqrt(jnp.mean(values * values, axis=-1, keepdims=True) + rms_eps) * gain


def up(n, m):
    return -(-n // m) * m


def call(body, out_shape, *args, **kw):
    return pl.pallas_call(body, out_shape=out_shape, **kw)(*args)


def core_order(core, own, other):
    return jnp.where(core == 0, own, other), jnp.where(core == 0, other, own)


def norm_body(res_ref, gain_ref, out_ref):
    groups, rows, part = out_ref.shape
    tp_rank = lax.axis_index("tp")
    res = res_ref[...].astype(f32)
    scale = lax.rsqrt(jnp.mean(res * res, axis=-1, keepdims=True) + rms_eps)
    own = pl.ds(pl.multiple_of(tp_rank * part, 128), part)
    half = (res_ref[:, own].astype(f32) * scale * gain_ref[:, own]).astype(bf16)
    half = jnp.concatenate([half, jnp.zeros((rows - half.shape[0], part), bf16)], axis=0)
    for g in range(groups):
        out_ref[g] = half


def proj_body(x_ref, own_ref, oth_ref, out_ref):
    groups, rows, part = x_ref.shape
    core = lax.axis_index("c")
    x = x_ref[...].reshape(groups * rows, part)
    pieces = []
    for p in range(own_ref.shape[0]):
        pieces += core_order(core, dot(x, own_ref[p]), dot(x, oth_ref[p]))
    y = jnp.concatenate(pieces, axis=1).astype(bf16).reshape(groups, rows, -1)
    for t in range(out_ref.shape[1]):
        out_ref[:, t] = y


def recur_body(recv_ref, lower_ref, gain_ref, state_ref, new_ref, out_ref, proj, act):
    groups, tp_count, rows, _ = recv_ref.shape
    seqs, _, size, _ = state_ref.shape
    heads = proj.shape[1]
    step = pl.program_id(0)

    @pl.when(step == 0)
    def _():
        pieces = groups // tp_count
        first = lax.axis_index("tp") * pieces
        blocks = [recv_ref[first + g].astype(f32).sum(axis=0) for g in range(pieces)]
        wide = blocks[0].shape[1] // 4
        for p in range(4):
            full = jnp.concatenate([b[:, p * wide : (p + 1) * wide] for b in blocks], axis=1)
            full = full.astype(bf16).astype(f32)
            for h in range(heads):
                proj[p, h] = full[:, h * size : (h + 1) * size]

    lower = lower_ref[step]
    query = jax.nn.silu(proj[0, step])
    forget = lower + (1.0 - lower) * jax.nn.sigmoid(proj[1, step])
    key = 1.0 - forget
    value = proj[2, step]
    mixed = query * forget
    high = mixed.astype(bf16)
    low = (mixed - high.astype(f32)).astype(bf16)
    lhs = jnp.concatenate([high, low], axis=0)
    forget_t = forget.T
    key_t = key.T
    row_ids = lax.broadcasted_iota(jnp.int32, (rows, size), 0)
    readout = jnp.sum(query * key, axis=1, keepdims=True) * value
    for s in range(seqs):
        old = state_ref[s, 0]
        both = dot(lhs, old)
        readout += jnp.where(row_ids == s, both[:rows] + both[rows:], 0.0)
        new_ref[s, 0] = (
            forget_t[:, s : s + 1] * old.astype(f32) + key_t[:, s : s + 1] * value[s : s + 1]
        ).astype(bf16)
    heads_out = rms_scale(readout, gain_ref[...]) * jax.nn.silu(proj[3, step])
    act[step] = heads_out.astype(bf16)

    @pl.when(step == heads - 1)
    def _():
        full = jnp.concatenate([act[h] for h in range(heads)], axis=1)
        for g in range(out_ref.shape[0]):
            out_ref[g] = full


def mix_body(x_ref, own_ref, oth_ref, out_ref):
    groups, rows, part = x_ref.shape
    x = x_ref[...].reshape(groups * rows, part)
    y = jnp.concatenate(
        core_order(lax.axis_index("c"), dot(x, own_ref[...]), dot(x, oth_ref[...])), axis=1
    )
    y = y.astype(bf16).reshape(groups, rows, -1)
    for t in range(out_ref.shape[1]):
        out_ref[:, t] = y


def slots_of(ids, width, slots, experts):
    seqs, tops = ids.shape
    column = lax.broadcasted_iota(jnp.int32, (seqs, width), 1)
    expert, place = column // slots, column % slots
    named = [ids[:, k : k + 1] == expert for k in range(tops)]
    names = sum(n.astype(f32) for n in named)
    before = (
        lax.broadcasted_iota(jnp.int32, (seqs, seqs), 0)
        > lax.broadcasted_iota(jnp.int32, (seqs, seqs), 1)
    ).astype(f32)
    rank = dot(before.astype(bf16), names.astype(bf16))
    here = jnp.where(rank == place.astype(f32), names, 0.0)
    return here, named


def dispatch_body(recv_ref, res_ref, gain_ref, ids_ref, out_ref, own_ref):
    groups, tp_count, rows, _ = recv_ref.shape
    seqs, width = res_ref.shape
    experts, slots, _ = out_ref.shape
    mixed = jnp.concatenate(
        [recv_ref[g].astype(f32).sum(axis=0) for g in range(groups)], axis=1
    )[:seqs]
    after = (res_ref[...].astype(f32) + mixed).astype(bf16).astype(f32)
    normed = rms_scale(after, gain_ref[...]).astype(bf16)
    here, _ = slots_of(ids_ref[...], experts * slots, slots, experts)
    picked = lax.dot_general(
        here.astype(bf16), normed, (((0,), (0,)), ((), ())), preferred_element_type=f32
    )
    out_ref[...] = picked.astype(bf16).reshape(experts, slots, width)
    part = own_ref.shape[1]
    own = after[:, :part]
    for t in range(1, tp_count):
        own = jnp.where(lax.axis_index("tp") == t, after[:, t * part : (t + 1) * part], own)
    own_ref[...] = own


def expert_body(x_ref, gate_ref, up_ref, down_ref, out_ref):
    sources, tp_count, slots, part = out_ref.shape
    x = x_ref[...].reshape(sources * slots, tp_count * part)
    hidden = (jax.nn.silu(dot(x, gate_ref[0])) * dot(x, up_ref[0])).astype(bf16)
    y = dot(hidden, down_ref[0]).astype(bf16)
    for t in range(tp_count):
        out_ref[:, t] = y[:, t * part : (t + 1) * part].reshape(sources, slots, part)


def combine_body(back_ref, ids_ref, weight_ref, own_ref, out_ref):
    experts, tp_count, slots, part = back_ref.shape
    rows = back_ref[:, 0].astype(f32)
    for t in range(1, tp_count):
        rows += back_ref[:, t].astype(f32)
    rows = rows.astype(bf16).reshape(experts * slots, part)
    here, named = slots_of(ids_ref[...], experts * slots, slots, experts)
    weight = sum(
        jnp.where(n, weight_ref[:, k : k + 1], 0.0) for k, n in enumerate(named)
    )
    weight = weight * here
    high = weight.astype(bf16)
    low = (weight - high.astype(f32)).astype(bf16)
    out_ref[...] = (own_ref[...] + dot(high, rows) + dot(low, rows)).astype(bf16)


def shards(
    residual_in,
    rec_state,
    mix_gain,
    w_query,
    w_forget,
    w_input,
    w_gate,
    lower_bound,
    head_gain,
    w_out,
    ffn_gain,
    route_ids,
    route_weight,
    expert_gate,
    expert_up,
    expert_down,
):
    groups, cores, tp_count = (lax.axis_size(a) for a in ("g", "c", "tp"))
    seqs, width = residual_in.shape
    part = width // tp_count
    cols = w_query.shape[1]
    _, heads, size, _ = rec_state.shape
    rows = up(seqs, 16)
    sds = jax.ShapeDtypeStruct

    own_w = jnp.stack([w_query, w_forget, w_input, w_gate, w_out])
    swap = [(i, i ^ 1) for i in range(cores)]
    oth_w = lax.ppermute(own_w, "c", swap)

    spread = call(
        norm_body, sds((groups, rows, part), bf16), residual_in, mix_gain.reshape(1, width)
    )
    gathered = lax.all_to_all(spread, "g", 0, 0, tiled=True)
    partial = call(
        proj_body,
        sds((groups, tp_count, rows, 4 * cores * cols), bf16),
        gathered,
        own_w[:4],
        oth_w[:4],
    )
    arrived = lax.all_to_all(
        partial.reshape(groups * tp_count, rows, -1), ("g", "tp"), 0, 0, tiled=True
    ).reshape(partial.shape)

    whole = lambda shape: pl.BlockSpec(shape, lambda i: (0,) * len(shape))
    per_head = pl.BlockSpec((seqs, 1, size, size), lambda i: (0, i, 0, 0))
    new_state, spread_heads = pl.pallas_call(
        recur_body,
        grid=(heads,),
        in_specs=[
            whole(arrived.shape),
            whole((heads, 1, size)),
            whole((1, size)),
            per_head,
        ],
        out_specs=[per_head, whole((groups, rows, heads * size))],
        out_shape=[sds(rec_state.shape, bf16), sds((groups, rows, heads * size), bf16)],
        scratch_shapes=[
            pltpu.VMEM((4, heads, rows, size), f32),
            pltpu.VMEM((heads, rows, size), bf16),
        ],
    )(arrived, lower_bound.reshape(heads, 1, size), head_gain.reshape(1, size), rec_state)

    all_heads = lax.all_to_all(spread_heads, "g", 0, 0, tiled=True)
    partial_mix = call(
        mix_body,
        sds((groups, tp_count, rows, cores * cols), bf16),
        all_heads,
        own_w[4],
        oth_w[4],
    )
    mix_home = lax.all_to_all(
        partial_mix.reshape(groups * tp_count, rows, -1), ("g", "tp"), 0, 0, tiled=True
    ).reshape(partial_mix.shape)

    experts = groups * cores * expert_gate.shape[0]
    capacity = max(2, seqs * route_ids.shape[1] // experts + 1)
    slots = up(capacity, 8)
    buffer, own_mix = call(
        dispatch_body,
        [sds((experts, slots, width), bf16), sds((seqs, part), f32)],
        mix_home,
        residual_in,
        ffn_gain.reshape(1, width),
        route_ids,
    )
    received = lax.all_to_all(buffer, ("g", "c"), 0, 0, tiled=True)
    down = call(
        expert_body,
        sds((experts, tp_count, slots, part), bf16),
        received,
        expert_gate,
        expert_up,
        expert_down,
    )
    back = lax.all_to_all(
        down.reshape(experts * tp_count, slots, part), ("g", "c", "tp"), 0, 0, tiled=True
    ).reshape(down.shape)
    layer_out = call(
        combine_body, sds((seqs, part), bf16), back, route_ids, route_weight, own_mix
    )
    return layer_out, new_state


def solution(mesh):
    ep, tp = mesh.shape["ep"], mesh.shape["tp"]
    split = Mesh(mesh.devices.reshape(ep // 2, 2, tp), ("g", "c", "tp"))
    seq = ("g", "c")
    in_specs = (
        P(seq, None),
        P(seq, "tp", None, None),
        P(),
        P("tp", seq),
        P("tp", seq),
        P("tp", seq),
        P("tp", seq),
        P("tp"),
        P(),
        P("tp", seq),
        P(),
        P(seq, None),
        P(seq, None),
        P(seq, None, "tp"),
        P(seq, None, "tp"),
        P(seq, "tp", None),
    )
    out_specs = (P(seq, "tp"), P(seq, "tp", None, None))
    return jax.shard_map(
        shards, mesh=split, in_specs=in_specs, out_specs=out_specs, check_vma=False
    )
```

```python
import functools

import jax
import jax.numpy as jnp
from jax import lax
from jax.experimental import pallas as pl
from jax.experimental.pallas import tpu as pltpu
from jax.sharding import Mesh, PartitionSpec as P

rms_eps = 1e-06
bf16, f32 = jnp.bfloat16, jnp.float32


def dot(a, b):
    return jnp.dot(a, b, preferred_element_type=f32)


def rms_scale(values, gain):
    return values * lax.rsqrt(jnp.mean(values * values, axis=-1, keepdims=True) + rms_eps) * gain


def up(n, m):
    return -(-n // m) * m


def call(body, out_shape, *args, mib=16, cost=None, **kw):
    return pl.pallas_call(
        body,
        out_shape=out_shape,
        compiler_params=pltpu.CompilerParams(vmem_limit_bytes=mib << 20),
        cost_estimate=cost,
        **kw,
    )(*args)


def dot_t(a, b):
    return lax.dot_general(a, b, (((1,), (1,)), ((), ())), preferred_element_type=f32)


def pick_part(rank, full, part):
    own = full[:, :part]
    for t in range(1, full.shape[1] // part):
        own = jnp.where(rank == t, full[:, t * part : (t + 1) * part], own)
    return own


def core_order(core, own, other):
    return jnp.where(core == 0, own, other), jnp.where(core == 0, other, own)


def norm_body(*refs):
    sources, (out_ref, own_ref, res_ref, gain_ref, sems) = refs[:7], refs[7:]
    targets = [res_ref, gain_ref] + [own_ref.at[p] for p in range(5)]
    loads = [
        pltpu.make_async_copy(source, target, sems.at[i])
        for i, (source, target) in enumerate(zip(sources, targets))
    ]
    for load in loads:
        load.start()
    groups, rows, part = out_ref.shape
    tp_rank = lax.axis_index("tp")
    for load in loads[:2]:
        load.wait()
    res = res_ref[...].astype(f32)
    scale = lax.rsqrt(jnp.mean(res * res, axis=-1, keepdims=True) + rms_eps)
    normed = (res * scale * gain_ref[...].reshape(1, -1)).astype(bf16)
    half = pick_part(tp_rank, normed, part)
    half = jnp.concatenate([half, jnp.zeros((rows - half.shape[0], part), bf16)], axis=0)
    for g in range(groups):
        out_ref[g] = half
    for load in loads[2:]:
        load.wait()


def proj_body(x_ref, own_ref, oth_ref, out_ref):
    groups, rows, part = x_ref.shape
    half = out_ref.shape[-1] // 2
    x = x_ref[...].reshape(groups * rows, part)
    for i, w_ref in enumerate((own_ref, oth_ref)):
        columns = jnp.concatenate([w_ref[p] for p in range(4)], axis=0)
        y = dot_t(x, columns).astype(bf16).reshape(groups, rows, half)
        for t in range(out_ref.shape[1]):
            out_ref[:, t, :, i * half : (i + 1) * half] = y


def read_body(recv_ref, lower_ref, gain_ref, state_ref, out_ref, forget_ref, value_ref):
    groups, tp_count, rows, both = recv_ref.shape
    seqs, heads, size, _ = state_ref.shape
    pieces = groups // tp_count
    first = lax.axis_index("tp") * pieces
    core = lax.axis_index("c")
    blocks = [recv_ref[first + g].astype(f32).sum(axis=0) for g in range(pieces)]
    cols = both // 8
    proj = []
    for p in range(4):
        parts = []
        for block in blocks:
            own = block[:, p * cols : (p + 1) * cols]
            other = block[:, both // 2 + p * cols : both // 2 + (p + 1) * cols]
            parts += core_order(core, own, other)
        proj.append(jnp.concatenate(parts, axis=1).astype(bf16).astype(f32))
    query = jax.nn.silu(proj[0])
    lower = lower_ref[...].reshape(1, -1)
    forget = lower + (1.0 - lower) * jax.nn.sigmoid(proj[1])
    forget_ref[...] = forget
    value_ref[...] = proj[2]
    gate = jax.nn.silu(proj[3])
    gain = gain_ref[...].reshape(1, -1)
    mixed = query * forget
    high = mixed.astype(bf16)
    low = (mixed - high.astype(f32)).astype(bf16)
    direct = query * (1.0 - forget)
    row_ids = lax.broadcasted_iota(jnp.int32, (rows, size), 0)
    for h in range(heads):
        lanes = slice(h * size, (h + 1) * size)
        lhs = jnp.concatenate([high[:, lanes], low[:, lanes]], axis=0)
        readout = jnp.sum(direct[:, lanes], axis=1, keepdims=True) * proj[2][:, lanes]
        for s in range(seqs):
            both_parts = dot(lhs, state_ref[s, h])
            readout += jnp.where(row_ids == s, both_parts[:rows] + both_parts[rows:], 0.0)
        heads_out = (rms_scale(readout, gain) * gate[:, lanes]).astype(bf16)
        for g in range(groups):
            out_ref[g, :, lanes] = heads_out


def state_body(forget_ref, value_ref, state_ref, new_ref):
    seqs = state_ref.shape[0]
    forget_t = forget_ref[...].T
    key_t = 1.0 - forget_t
    value = value_ref[...]
    for s in range(seqs):
        new_ref[s, 0] = (
            forget_t[:, s : s + 1] * state_ref[s, 0].astype(f32)
            + key_t[:, s : s + 1] * value[s : s + 1]
        ).astype(bf16)


def mix_body(x_ref, own_ref, oth_ref, out_ref):
    groups, rows, part = x_ref.shape
    x = x_ref[...].reshape(groups * rows, part)
    pair = core_order(
        lax.axis_index("c"), dot_t(x, own_ref[4]), dot_t(x, oth_ref[4])
    )
    y = jnp.concatenate(pair, axis=1).astype(bf16).reshape(groups, rows, -1)
    for t in range(out_ref.shape[1]):
        out_ref[:, t] = y


def slots_of(ids, slots, experts):
    tops, seqs = ids.shape
    row = lax.broadcasted_iota(jnp.int32, (experts * slots, seqs), 0)
    expert, place = row // slots, row % slots
    named = [ids[k : k + 1] == expert for k in range(tops)]
    names = sum(n.astype(f32) for n in named)
    before = (
        lax.broadcasted_iota(jnp.int32, (seqs, seqs), 0)
        < lax.broadcasted_iota(jnp.int32, (seqs, seqs), 1)
    ).astype(f32)
    rank = dot(names.astype(bf16), before.astype(bf16))
    here = jnp.where(rank == place.astype(f32), names, 0.0)
    return here, named


def dispatch_body(recv_ref, res_ref, gain_ref, ids_ref, out_ref, own_ref):
    groups, tp_count, rows, _ = recv_ref.shape
    seqs, width = res_ref.shape
    experts, slots, _ = out_ref.shape
    mixed = jnp.concatenate(
        [recv_ref[g].astype(f32).sum(axis=0) for g in range(groups)], axis=1
    )[:seqs]
    after = (res_ref[...].astype(f32) + mixed).astype(bf16).astype(f32)
    normed = rms_scale(after, gain_ref[...].reshape(1, -1)).astype(bf16)
    here, _ = slots_of(ids_ref[...], slots, experts)
    out_ref[...] = dot(here.astype(bf16), normed).astype(bf16).reshape(experts, slots, width)
    own_ref[...] = pick_part(lax.axis_index("tp"), after, own_ref.shape[1])


def expert_body(x_ref, gate_ref, up_ref, down_ref, out_ref):
    sources, tp_count, slots, part = out_ref.shape
    x = x_ref[...].reshape(sources * slots, tp_count * part)
    hidden = (jax.nn.silu(dot(x, gate_ref[0])) * dot(x, up_ref[0])).astype(bf16)
    y = dot(hidden, down_ref[0]).astype(bf16)
    for t in range(tp_count):
        out_ref[:, t] = y[:, t * part : (t + 1) * part].reshape(sources, slots, part)


def combine_body(back_ref, ids_ref, weight_ref, own_ref, out_ref):
    experts, tp_count, slots, part = back_ref.shape
    rows = back_ref[:, 0].astype(f32)
    for t in range(1, tp_count):
        rows += back_ref[:, t].astype(f32)
    rows = rows.astype(bf16).reshape(experts * slots, part)
    here, named = slots_of(ids_ref[...], slots, experts)
    weight = sum(jnp.where(n, weight_ref[k : k + 1], 0.0) for k, n in enumerate(named))
    weight = weight * here
    high = weight.astype(bf16)
    low = (weight - high.astype(f32)).astype(bf16)
    total = sum(
        lax.dot_general(w, rows, (((0,), (0,)), ((), ())), preferred_element_type=f32)
        for w in (high, low)
    )
    out_ref[...] = (own_ref[...] + total).astype(bf16)


def shards(
    residual_in,
    rec_state,
    mix_gain,
    w_query,
    w_forget,
    w_input,
    w_gate,
    lower_bound,
    head_gain,
    w_out,
    ffn_gain,
    route_ids,
    route_weight,
    expert_gate,
    expert_up,
    expert_down,
):
    groups, cores, tp_count = (lax.axis_size(a) for a in ("g", "c", "tp"))
    seqs, width = residual_in.shape
    part = width // tp_count
    cols = w_query.shape[1]
    _, heads, size, _ = rec_state.shape
    rows = up(seqs, 16)
    sds = jax.ShapeDtypeStruct

    vmem, hbm = (pl.BlockSpec(memory_space=m) for m in (pltpu.VMEM, pltpu.HBM))
    spread, own_w = call(
        norm_body,
        [sds((groups, rows, part), bf16), sds((5, cols, part), bf16)],
        residual_in,
        mix_gain,
        *(w.T for w in (w_query, w_forget, w_input, w_gate, w_out)),
        mib=60,
        in_specs=[hbm] * 7,
        out_specs=[vmem, vmem],
        scratch_shapes=[
            pltpu.VMEM(residual_in.shape, bf16),
            pltpu.VMEM(mix_gain.shape, f32),
            pltpu.SemaphoreType.DMA((7,)),
        ],
    )
    oth_w = lax.ppermute(own_w, "c", [(i, i ^ 1) for i in range(cores)])
    gathered = lax.all_to_all(spread, "g", 0, 0, tiled=True)

    partial = call(
        proj_body,
        sds((groups, tp_count, rows, 4 * cores * cols), bf16),
        gathered,
        own_w,
        oth_w,
    )
    arrived = lax.all_to_all(
        partial.reshape(groups * tp_count, rows, -1), ("g", "tp"), 0, 0, tiled=True
    ).reshape(partial.shape)

    spread_heads, forget, value = call(
        read_body,
        [
            sds((groups, rows, heads * size), bf16),
            sds((rows, heads * size), f32),
            sds((rows, heads * size), f32),
        ],
        arrived,
        lower_bound,
        head_gain,
        rec_state,
    )
    all_heads = lax.all_to_all(spread_heads, "g", 0, 0, tiled=True)

    per_head = pl.BlockSpec((seqs, 1, size, size), lambda i: (0, i, 0, 0))
    head_lanes = pl.BlockSpec((rows, size), lambda i: (0, i))
    new_state = call(
        state_body,
        sds(rec_state.shape, bf16),
        forget,
        value,
        rec_state,
        grid=(heads,),
        in_specs=[head_lanes, head_lanes, per_head],
        out_specs=per_head,
        cost=pl.CostEstimate(
            flops=10**7, bytes_accessed=4 * rec_state.size, transcendentals=0
        ),
    )

    partial_mix = call(
        mix_body, sds((groups, tp_count, rows, cores * cols), bf16), all_heads, own_w, oth_w
    )
    mix_home = lax.all_to_all(
        partial_mix.reshape(groups * tp_count, rows, -1), ("g", "tp"), 0, 0, tiled=True
    ).reshape(partial_mix.shape)

    experts = groups * cores * expert_gate.shape[0]
    capacity = max(2, seqs * route_ids.shape[1] // experts + 1)
    slots = up(capacity, 8)
    buffer, own_mix = call(
        dispatch_body,
        [sds((experts, slots, width), bf16), sds((seqs, part), f32)],
        mix_home,
        residual_in,
        ffn_gain,
        route_ids.T,
    )
    received = lax.all_to_all(buffer, ("g", "c"), 0, 0, tiled=True)
    down = call(
        expert_body,
        sds((experts, tp_count, slots, part), bf16),
        received,
        expert_gate,
        expert_up,
        expert_down,
    )
    back = lax.all_to_all(
        down.reshape(experts * tp_count, slots, part), ("g", "c", "tp"), 0, 0, tiled=True
    ).reshape(down.shape)
    layer_out = call(
        combine_body, sds((seqs, part), bf16), back, route_ids.T, route_weight.T, own_mix
    )
    return layer_out, new_state


def solution(mesh):
    ep, tp = mesh.shape["ep"], mesh.shape["tp"]
    split = Mesh(mesh.devices.reshape(ep // 2, 2, tp), ("g", "c", "tp"))
    seq = ("g", "c")
    in_specs = (
        P(seq, None),
        P(seq, "tp", None, None),
        P(),
        P("tp", seq),
        P("tp", seq),
        P("tp", seq),
        P("tp", seq),
        P("tp"),
        P(),
        P("tp", seq),
        P(),
        P(seq, None),
        P(seq, None),
        P(seq, None, "tp"),
        P(seq, None, "tp"),
        P(seq, "tp", None),
    )
    out_specs = (P(seq, "tp"), P(seq, "tp", None, None))
    return jax.shard_map(
        shards, mesh=split, in_specs=in_specs, out_specs=out_specs, check_vma=False
    )
```

```python
import functools

import jax
import jax.numpy as jnp
from jax import lax
from jax.experimental import pallas as pl
from jax.experimental.pallas import tpu as pltpu
from jax.sharding import Mesh, PartitionSpec as P

rms_eps = 1e-06
bf16, f32 = jnp.bfloat16, jnp.float32


def dot(a, b):
    return jnp.dot(a, b, preferred_element_type=f32)


def rms_scale(values, gain):
    return values * lax.rsqrt(jnp.mean(values * values, axis=-1, keepdims=True) + rms_eps) * gain


def up(n, m):
    return -(-n // m) * m


def call(body, out_shape, *args, mib=16, cost=None, **kw):
    return pl.pallas_call(
        body,
        out_shape=out_shape,
        compiler_params=pltpu.CompilerParams(vmem_limit_bytes=mib << 20),
        cost_estimate=cost,
        **kw,
    )(*args)


def dot_t(a, b):
    return lax.dot_general(a, b, (((1,), (1,)), ((), ())), preferred_element_type=f32)


def pick_part(rank, full, part):
    own = full[:, :part]
    for t in range(1, full.shape[1] // part):
        own = jnp.where(rank == t, full[:, t * part : (t + 1) * part], own)
    return own


def core_order(core, own, other):
    return jnp.where(core == 0, own, other), jnp.where(core == 0, other, own)


def norm_body(*refs):
    sources, (out_ref, own_ref, res_ref, gain_ref, sems) = refs[:7], refs[7:]
    targets = [res_ref, gain_ref] + [own_ref.at[p] for p in range(5)]
    loads = [
        pltpu.make_async_copy(source, target, sems.at[i])
        for i, (source, target) in enumerate(zip(sources, targets))
    ]
    for load in loads:
        load.start()
    groups, rows, part = out_ref.shape
    tp_rank = lax.axis_index("tp")
    for load in loads[:2]:
        load.wait()
    res = res_ref[...].astype(f32)
    scale = lax.rsqrt(jnp.mean(res * res, axis=-1, keepdims=True) + rms_eps)
    normed = (res * scale * gain_ref[...].reshape(1, -1)).astype(bf16)
    half = pick_part(tp_rank, normed, part)
    half = jnp.concatenate([half, jnp.zeros((rows - half.shape[0], part), bf16)], axis=0)
    for g in range(groups):
        out_ref[g] = half
    for load in loads[2:]:
        load.wait()


def proj_body(x_ref, own_ref, oth_ref, out_ref):
    groups, rows, part = x_ref.shape
    half = out_ref.shape[-1] // 2
    x = x_ref[...].reshape(groups * rows, part)
    for i, w_ref in enumerate((own_ref, oth_ref)):
        columns = jnp.concatenate([w_ref[p] for p in range(4)], axis=0)
        y = dot_t(x, columns).astype(bf16).reshape(groups, rows, half)
        for t in range(out_ref.shape[1]):
            out_ref[:, t, :, i * half : (i + 1) * half] = y


def read_body(recv_ref, lower_ref, gain_ref, state_ref, out_ref, forget_ref, value_ref):
    groups, tp_count, rows, both = recv_ref.shape
    seqs, heads, size, _ = state_ref.shape
    pieces = groups // tp_count
    first = lax.axis_index("tp") * pieces
    core = lax.axis_index("c")
    blocks = [recv_ref[first + g].astype(f32).sum(axis=0) for g in range(pieces)]
    cols = both // 8
    proj = []
    for p in range(4):
        parts = []
        for block in blocks:
            own = block[:, p * cols : (p + 1) * cols]
            other = block[:, both // 2 + p * cols : both // 2 + (p + 1) * cols]
            parts += core_order(core, own, other)
        proj.append(jnp.concatenate(parts, axis=1).astype(bf16).astype(f32))
    query = jax.nn.silu(proj[0])
    lower = lower_ref[...].reshape(1, -1)
    forget = lower + (1.0 - lower) * jax.nn.sigmoid(proj[1])
    forget_ref[...] = forget
    value_ref[...] = proj[2]
    gate = jax.nn.silu(proj[3])
    gain = gain_ref[...].reshape(1, -1)
    mixed = query * forget
    high = mixed.astype(bf16)
    low = (mixed - high.astype(f32)).astype(bf16)
    direct = query * (1.0 - forget)
    row_ids = lax.broadcasted_iota(jnp.int32, (rows, size), 0)
    for h in range(heads):
        lanes = slice(h * size, (h + 1) * size)
        lhs = jnp.concatenate([high[:, lanes], low[:, lanes]], axis=0)
        readout = jnp.sum(direct[:, lanes], axis=1, keepdims=True) * proj[2][:, lanes]
        for s in range(seqs):
            both_parts = dot(lhs, state_ref[s, h])
            readout += jnp.where(row_ids == s, both_parts[:rows] + both_parts[rows:], 0.0)
        heads_out = (rms_scale(readout, gain) * gate[:, lanes]).astype(bf16)
        for g in range(groups):
            out_ref[g, :, lanes] = heads_out


def state_body(forget_ref, value_ref, state_ref, new_ref):
    seqs = state_ref.shape[0]
    forget_t = forget_ref[...].T
    key_t = 1.0 - forget_t
    value = value_ref[...]
    for s in range(seqs):
        new_ref[s, 0] = (
            forget_t[:, s : s + 1] * state_ref[s, 0].astype(f32)
            + key_t[:, s : s + 1] * value[s : s + 1]
        ).astype(bf16)


def mix_body(x_ref, own_ref, oth_ref, out_ref):
    groups, rows, part = x_ref.shape
    x = x_ref[...].reshape(groups * rows, part)
    pair = core_order(
        lax.axis_index("c"), dot_t(x, own_ref[4]), dot_t(x, oth_ref[4])
    )
    y = jnp.concatenate(pair, axis=1).astype(bf16).reshape(groups, rows, -1)
    for t in range(out_ref.shape[1]):
        out_ref[:, t] = y


def slots_of(ids, slots, experts):
    tops, seqs = ids.shape
    row = lax.broadcasted_iota(jnp.int32, (experts * slots, seqs), 0)
    expert, place = row // slots, row % slots
    named = [ids[k : k + 1] == expert for k in range(tops)]
    names = sum(n.astype(f32) for n in named)
    before = (
        lax.broadcasted_iota(jnp.int32, (seqs, seqs), 0)
        < lax.broadcasted_iota(jnp.int32, (seqs, seqs), 1)
    ).astype(f32)
    rank = dot(names.astype(bf16), before.astype(bf16))
    here = jnp.where(rank == place.astype(f32), names, 0.0)
    return here, named


def dispatch_body(recv_ref, res_ref, gain_ref, ids_ref, out_ref, own_ref):
    groups, tp_count, rows, _ = recv_ref.shape
    seqs, width = res_ref.shape
    experts, slots, _ = out_ref.shape
    mixed = jnp.concatenate(
        [recv_ref[g].astype(f32).sum(axis=0) for g in range(groups)], axis=1
    )[:seqs]
    after = (res_ref[...].astype(f32) + mixed).astype(bf16).astype(f32)
    normed = rms_scale(after, gain_ref[...].reshape(1, -1)).astype(bf16)
    here, _ = slots_of(ids_ref[...], slots, experts)
    out_ref[...] = dot(here.astype(bf16), normed).astype(bf16).reshape(experts, slots, width)
    own_ref[...] = pick_part(lax.axis_index("tp"), after, own_ref.shape[1])


def expert_body(x_ref, gate_ref, up_ref, down_ref, out_ref):
    sources, tp_count, slots, part = out_ref.shape
    x = x_ref[...].reshape(sources * slots, tp_count * part)
    hidden = (jax.nn.silu(dot(x, gate_ref[0])) * dot(x, up_ref[0])).astype(bf16)
    y = dot(hidden, down_ref[0]).astype(bf16)
    for t in range(tp_count):
        out_ref[:, t] = y[:, t * part : (t + 1) * part].reshape(sources, slots, part)


def combine_body(back_ref, ids_ref, weight_ref, own_ref, out_ref):
    experts, tp_count, slots, part = back_ref.shape
    rows = back_ref[:, 0].astype(f32)
    for t in range(1, tp_count):
        rows += back_ref[:, t].astype(f32)
    rows = rows.astype(bf16).reshape(experts * slots, part)
    here, named = slots_of(ids_ref[...], slots, experts)
    weight = sum(jnp.where(n, weight_ref[k : k + 1], 0.0) for k, n in enumerate(named))
    weight = weight * here
    high = weight.astype(bf16)
    low = (weight - high.astype(f32)).astype(bf16)
    total = sum(
        lax.dot_general(w, rows, (((0,), (0,)), ((), ())), preferred_element_type=f32)
        for w in (high, low)
    )
    out_ref[...] = (own_ref[...] + total).astype(bf16)


def shards(
    residual_in,
    rec_state,
    mix_gain,
    w_query,
    w_forget,
    w_input,
    w_gate,
    lower_bound,
    head_gain,
    w_out,
    ffn_gain,
    route_ids,
    route_weight,
    expert_gate,
    expert_up,
    expert_down,
):
    groups, cores, tp_count = (lax.axis_size(a) for a in ("g", "c", "tp"))
    seqs, width = residual_in.shape
    part = width // tp_count
    cols = w_query.shape[1]
    _, heads, size, _ = rec_state.shape
    rows = up(seqs, 16)
    sds = jax.ShapeDtypeStruct

    sources = [residual_in, mix_gain]
    sources += [w.T for w in (w_query, w_forget, w_input, w_gate, w_out)]
    vmem, hbm = (pl.BlockSpec(memory_space=m) for m in (pltpu.VMEM, pltpu.HBM))
    spread, own_w = call(
        norm_body,
        [sds((groups, rows, part), bf16), sds((5, cols, part), bf16)],
        *(pltpu.with_memory_space_constraint(a, pltpu.HBM) for a in sources),
        in_specs=[hbm] * 7,
        out_specs=[vmem, vmem],
        scratch_shapes=[
            pltpu.VMEM(residual_in.shape, bf16),
            pltpu.VMEM(mix_gain.shape, f32),
            pltpu.SemaphoreType.DMA((7,)),
        ],
    )
    oth_w = lax.ppermute(own_w, "c", [(i, i ^ 1) for i in range(cores)])
    gathered = lax.all_to_all(spread, "g", 0, 0, tiled=True)

    partial = call(
        proj_body,
        sds((groups, tp_count, rows, 4 * cores * cols), bf16),
        gathered,
        own_w,
        oth_w,
    )
    arrived = lax.all_to_all(
        partial.reshape(groups * tp_count, rows, -1), ("g", "tp"), 0, 0, tiled=True
    ).reshape(partial.shape)

    spread_heads, forget, value = call(
        read_body,
        [
            sds((groups, rows, heads * size), bf16),
            sds((rows, heads * size), f32),
            sds((rows, heads * size), f32),
        ],
        arrived,
        lower_bound,
        head_gain,
        rec_state,
    )
    all_heads = lax.all_to_all(spread_heads, "g", 0, 0, tiled=True)

    per_head = pl.BlockSpec((seqs, 1, size, size), lambda i: (0, i, 0, 0))
    head_lanes = pl.BlockSpec((rows, size), lambda i: (0, i))
    new_state = call(
        state_body,
        sds(rec_state.shape, bf16),
        forget,
        value,
        rec_state,
        grid=(heads,),
        in_specs=[head_lanes, head_lanes, per_head],
        out_specs=per_head,
        cost=pl.CostEstimate(
            flops=10**7, bytes_accessed=4 * rec_state.size, transcendentals=0
        ),
    )

    partial_mix = call(
        mix_body, sds((groups, tp_count, rows, cores * cols), bf16), all_heads, own_w, oth_w
    )
    mix_home = lax.all_to_all(
        partial_mix.reshape(groups * tp_count, rows, -1), ("g", "tp"), 0, 0, tiled=True
    ).reshape(partial_mix.shape)

    experts = groups * cores * expert_gate.shape[0]
    capacity = max(2, seqs * route_ids.shape[1] // experts + 1)
    slots = up(capacity, 8)
    buffer, own_mix = call(
        dispatch_body,
        [sds((experts, slots, width), bf16), sds((seqs, part), f32)],
        mix_home,
        residual_in,
        ffn_gain,
        route_ids.T,
    )
    received = lax.all_to_all(buffer, ("g", "c"), 0, 0, tiled=True)
    down = call(
        expert_body,
        sds((experts, tp_count, slots, part), bf16),
        received,
        expert_gate,
        expert_up,
        expert_down,
    )
    back = lax.all_to_all(
        down.reshape(experts * tp_count, slots, part), ("g", "c", "tp"), 0, 0, tiled=True
    ).reshape(down.shape)
    layer_out = call(
        combine_body, sds((seqs, part), bf16), back, route_ids.T, route_weight.T, own_mix
    )
    return layer_out, new_state


def solution(mesh):
    ep, tp = mesh.shape["ep"], mesh.shape["tp"]
    split = Mesh(mesh.devices.reshape(ep // 2, 2, tp), ("g", "c", "tp"))
    seq = ("g", "c")
    in_specs = (
        P(seq, None),
        P(seq, "tp", None, None),
        P(),
        P("tp", seq),
        P("tp", seq),
        P("tp", seq),
        P("tp", seq),
        P("tp"),
        P(),
        P("tp", seq),
        P(),
        P(seq, None),
        P(seq, None),
        P(seq, None, "tp"),
        P(seq, None, "tp"),
        P(seq, "tp", None),
    )
    out_specs = (P(seq, "tp"), P(seq, "tp", None, None))
    return jax.shard_map(
        shards, mesh=split, in_specs=in_specs, out_specs=out_specs, check_vma=False
    )
```

```python
import functools

import jax
import jax.numpy as jnp
from jax import lax
from jax.experimental import pallas as pl
from jax.experimental.pallas import tpu as pltpu
from jax.sharding import Mesh, PartitionSpec as P

rms_eps = 1e-06
bf16, f32 = jnp.bfloat16, jnp.float32


def dot(a, b):
    return jnp.dot(a, b, preferred_element_type=f32)


def rms_scale(values, gain):
    return values * lax.rsqrt(jnp.mean(values * values, axis=-1, keepdims=True) + rms_eps) * gain


def up(n, m):
    return -(-n // m) * m


def call(body, out_shape, *args, mib=16, cost=None, **kw):
    return pl.pallas_call(
        body,
        out_shape=out_shape,
        compiler_params=pltpu.CompilerParams(vmem_limit_bytes=mib << 20),
        cost_estimate=cost,
        **kw,
    )(*args)


def dot_t(a, b):
    return lax.dot_general(a, b, (((1,), (1,)), ((), ())), preferred_element_type=f32)


def pick_part(rank, full, part):
    own = full[:, :part]
    for t in range(1, full.shape[1] // part):
        own = jnp.where(rank == t, full[:, t * part : (t + 1) * part], own)
    return own


def core_order(core, own, other):
    return jnp.where(core == 0, own, other), jnp.where(core == 0, other, own)


def norm_body(*refs):
    sources, (out_ref, own_ref, res_ref, gain_ref, sems) = refs[:7], refs[7:]
    targets = [res_ref, gain_ref] + [own_ref.at[p] for p in range(5)]
    loads = [
        pltpu.make_async_copy(source, target, sems.at[i])
        for i, (source, target) in enumerate(zip(sources, targets))
    ]
    for load in loads:
        load.start()
    groups, rows, part = out_ref.shape
    tp_rank = lax.axis_index("tp")
    for load in loads[:2]:
        load.wait()
    res = res_ref[...].astype(f32)
    scale = lax.rsqrt(jnp.mean(res * res, axis=-1, keepdims=True) + rms_eps)
    normed = (res * scale * gain_ref[...].reshape(1, -1)).astype(bf16)
    half = pick_part(tp_rank, normed, part)
    half = jnp.concatenate([half, jnp.zeros((rows - half.shape[0], part), bf16)], axis=0)
    for g in range(groups):
        out_ref[g] = half
    for load in loads[2:]:
        load.wait()


def proj_body(x_ref, own_ref, oth_ref, out_ref):
    groups, rows, part = x_ref.shape
    half = out_ref.shape[-1] // 2
    x = x_ref[...].reshape(groups * rows, part)
    for i, w_ref in enumerate((own_ref, oth_ref)):
        columns = jnp.concatenate([w_ref[p] for p in range(4)], axis=0)
        y = dot_t(x, columns).astype(bf16).reshape(groups, rows, half)
        for t in range(out_ref.shape[1]):
            out_ref[:, t, :, i * half : (i + 1) * half] = y


def read_body(recv_ref, lower_ref, gain_ref, state_ref, out_ref, forget_ref, value_ref):
    groups, tp_count, rows, both = recv_ref.shape
    seqs, heads, size, _ = state_ref.shape
    pieces = groups // tp_count
    first = lax.axis_index("tp") * pieces
    core = lax.axis_index("c")
    blocks = [recv_ref[first + g].astype(f32).sum(axis=0) for g in range(pieces)]
    cols = both // 8
    proj = []
    for p in range(4):
        parts = []
        for block in blocks:
            own = block[:, p * cols : (p + 1) * cols]
            other = block[:, both // 2 + p * cols : both // 2 + (p + 1) * cols]
            parts += core_order(core, own, other)
        proj.append(jnp.concatenate(parts, axis=1).astype(bf16).astype(f32))
    query = jax.nn.silu(proj[0])
    lower = lower_ref[...].reshape(1, -1)
    forget = lower + (1.0 - lower) * jax.nn.sigmoid(proj[1])
    forget_ref[...] = forget
    value_ref[...] = proj[2]
    gate = jax.nn.silu(proj[3])
    gain = gain_ref[...].reshape(1, -1)
    mixed = query * forget
    high = mixed.astype(bf16)
    low = (mixed - high.astype(f32)).astype(bf16)
    direct = query * (1.0 - forget)
    row_ids = lax.broadcasted_iota(jnp.int32, (rows, size), 0)
    for h in range(heads):
        lanes = slice(h * size, (h + 1) * size)
        lhs = jnp.concatenate([high[:, lanes], low[:, lanes]], axis=0)
        readout = jnp.sum(direct[:, lanes], axis=1, keepdims=True) * proj[2][:, lanes]
        for s in range(seqs):
            both_parts = dot(lhs, state_ref[s, h])
            readout += jnp.where(row_ids == s, both_parts[:rows] + both_parts[rows:], 0.0)
        heads_out = (rms_scale(readout, gain) * gate[:, lanes]).astype(bf16)
        for g in range(groups):
            out_ref[g, :, lanes] = heads_out


def state_body(forget_ref, value_ref, state_ref, new_ref):
    seqs = state_ref.shape[0]
    forget_t = forget_ref[...].T
    key_t = 1.0 - forget_t
    value = value_ref[...]
    for s in range(seqs):
        new_ref[s, 0] = (
            forget_t[:, s : s + 1] * state_ref[s, 0].astype(f32)
            + key_t[:, s : s + 1] * value[s : s + 1]
        ).astype(bf16)


def mix_body(x_ref, own_ref, oth_ref, out_ref):
    groups, rows, part = x_ref.shape
    x = x_ref[...].reshape(groups * rows, part)
    pair = core_order(
        lax.axis_index("c"), dot_t(x, own_ref[4]), dot_t(x, oth_ref[4])
    )
    y = jnp.concatenate(pair, axis=1).astype(bf16).reshape(groups, rows, -1)
    for t in range(out_ref.shape[1]):
        out_ref[:, t] = y


def slots_of(ids, slots, experts):
    tops, seqs = ids.shape
    row = lax.broadcasted_iota(jnp.int32, (experts * slots, seqs), 0)
    expert, place = row // slots, row % slots
    named = [ids[k : k + 1] == expert for k in range(tops)]
    names = sum(n.astype(f32) for n in named)
    before = (
        lax.broadcasted_iota(jnp.int32, (seqs, seqs), 0)
        < lax.broadcasted_iota(jnp.int32, (seqs, seqs), 1)
    ).astype(f32)
    rank = dot(names.astype(bf16), before.astype(bf16))
    here = jnp.where(rank == place.astype(f32), names, 0.0)
    return here, named


def dispatch_body(recv_ref, res_ref, gain_ref, ids_ref, out_ref, own_ref, lines):
    groups, tp_count, rows, _ = recv_ref.shape
    seqs, width = res_ref.shape
    per_row = width // 128
    slots_all = out_ref.shape[0] // per_row
    experts = groups * lax.axis_size("c")
    mixed = jnp.concatenate(
        [recv_ref[g].astype(f32).sum(axis=0) for g in range(groups)], axis=1
    )[:seqs]
    after = (res_ref[...].astype(f32) + mixed).astype(bf16).astype(f32)
    normed = rms_scale(after, gain_ref[...].reshape(1, -1)).astype(bf16)
    here, _ = slots_of(ids_ref[...], slots_all // experts, experts)
    picked = dot(here.astype(bf16), normed)
    for j in range(per_row):
        lines[pl.ds(j, slots_all, stride=per_row), :] = picked[:, j * 128 : (j + 1) * 128]
    out_ref[...] = lines[...].astype(bf16)
    own_ref[...] = pick_part(lax.axis_index("tp"), after, own_ref.shape[1])


def expert_body(capacity, x_ref, gate_ref, up_ref, down_ref, out_ref, lines, sent):
    width = gate_ref.shape[1]
    per_row = width // 128
    count = x_ref.shape[0]
    sources = count // (capacity * per_row)
    lines[:count] = x_ref[...].astype(f32)
    lines[count:] = jnp.zeros((lines.shape[0] - count, 128), f32)
    x = jnp.concatenate(
        [
            jnp.concatenate(
                [
                    lines[pl.ds(e * capacity * per_row + j, 8, stride=per_row), :]
                    for j in range(per_row)
                ],
                axis=1,
            )
            for e in range(sources)
        ],
        axis=0,
    ).astype(bf16)
    hidden = (jax.nn.silu(dot(x, gate_ref[0])) * dot(x, up_ref[0])).astype(bf16)
    y = dot(hidden, down_ref[0])
    targets, chunk, _ = out_ref.shape
    tp_count = targets // sources
    per_part = per_row // tp_count
    for d in range(targets):
        e, t = d // tp_count, d % tp_count
        for j in range(per_part):
            lane = (t * per_part + j) * 128
            sent[pl.ds(d * chunk + j, 8, stride=per_part), :] = y[
                e * 8 : (e + 1) * 8, lane : lane + 128
            ]
    for d in range(targets):
        out_ref[d] = sent[d * chunk : (d + 1) * chunk].astype(bf16)


def combine_body(back_ref, ids_ref, weight_ref, own_ref, out_ref, lines):
    targets, chunk, _ = back_ref.shape
    tp_count = lax.axis_size("tp")
    experts = targets // tp_count
    per_part = own_ref.shape[1] // 128
    for d in range(targets):
        lines[d * chunk : (d + 1) * chunk] = back_ref[d].astype(f32)
    lines[targets * chunk :] = jnp.zeros((lines.shape[0] - targets * chunk, 128), f32)

    def piece(e, j):
        return sum(
            lines[pl.ds((e * tp_count + t) * chunk + j, 8, stride=per_part), :]
            for t in range(tp_count)
        )

    rows = jnp.concatenate(
        [
            jnp.concatenate([piece(e, j) for j in range(per_part)], axis=1)
            for e in range(experts)
        ],
        axis=0,
    ).astype(bf16)
    here, named = slots_of(ids_ref[...], 8, experts)
    weight = sum(jnp.where(n, weight_ref[k : k + 1], 0.0) for k, n in enumerate(named))
    weight = weight * here
    high = weight.astype(bf16)
    low = (weight - high.astype(f32)).astype(bf16)
    total = sum(
        lax.dot_general(w, rows, (((0,), (0,)), ((), ())), preferred_element_type=f32)
        for w in (high, low)
    )
    out_ref[...] = (own_ref[...] + total).astype(bf16)


def capacity_of(seqs, tops, experts):
    return max(2, seqs * tops // experts + 1)


def shards(
    residual_in,
    rec_state,
    mix_gain,
    w_query,
    w_forget,
    w_input,
    w_gate,
    lower_bound,
    head_gain,
    w_out,
    ffn_gain,
    route_ids,
    route_weight,
    expert_gate,
    expert_up,
    expert_down,
):
    groups, cores, tp_count = (lax.axis_size(a) for a in ("g", "c", "tp"))
    seqs, width = residual_in.shape
    part = width // tp_count
    cols = w_query.shape[1]
    _, heads, size, _ = rec_state.shape
    rows = up(seqs, 16)
    sds = jax.ShapeDtypeStruct

    sources = [residual_in, mix_gain]
    sources += [w.T for w in (w_query, w_forget, w_input, w_gate, w_out)]
    vmem, hbm = (pl.BlockSpec(memory_space=m) for m in (pltpu.VMEM, pltpu.HBM))
    spread, own_w = call(
        norm_body,
        [sds((groups, rows, part), bf16), sds((5, cols, part), bf16)],
        *(pltpu.with_memory_space_constraint(a, pltpu.HBM) for a in sources),
        in_specs=[hbm] * 7,
        out_specs=[vmem, vmem],
        scratch_shapes=[
            pltpu.VMEM(residual_in.shape, bf16),
            pltpu.VMEM(mix_gain.shape, f32),
            pltpu.SemaphoreType.DMA((7,)),
        ],
    )
    oth_w = lax.ppermute(own_w, "c", [(i, i ^ 1) for i in range(cores)])
    gathered = lax.all_to_all(spread, "g", 0, 0, tiled=True)

    partial = call(
        proj_body,
        sds((groups, tp_count, rows, 4 * cores * cols), bf16),
        gathered,
        own_w,
        oth_w,
    )
    arrived = lax.all_to_all(
        partial.reshape(groups * tp_count, rows, -1), ("g", "tp"), 0, 0, tiled=True
    ).reshape(partial.shape)

    spread_heads, forget, value = call(
        read_body,
        [
            sds((groups, rows, heads * size), bf16),
            sds((rows, heads * size), f32),
            sds((rows, heads * size), f32),
        ],
        arrived,
        lower_bound,
        head_gain,
        rec_state,
    )
    all_heads = lax.all_to_all(spread_heads, "g", 0, 0, tiled=True)

    per_head = pl.BlockSpec((seqs, 1, size, size), lambda i: (0, i, 0, 0))
    head_lanes = pl.BlockSpec((rows, size), lambda i: (0, i))
    new_state = call(
        state_body,
        sds(rec_state.shape, bf16),
        forget,
        value,
        rec_state,
        grid=(heads,),
        in_specs=[head_lanes, head_lanes, per_head],
        out_specs=per_head,
        cost=pl.CostEstimate(
            flops=10**7, bytes_accessed=4 * rec_state.size, transcendentals=0
        ),
    )

    partial_mix = call(
        mix_body, sds((groups, tp_count, rows, cores * cols), bf16), all_heads, own_w, oth_w
    )
    mix_home = lax.all_to_all(
        partial_mix.reshape(groups * tp_count, rows, -1), ("g", "tp"), 0, 0, tiled=True
    ).reshape(partial_mix.shape)

    experts = groups * cores
    capacity = capacity_of(seqs, route_ids.shape[1], experts)
    assert capacity <= 8
    lines = experts * capacity * width // 128
    buffer, own_mix = call(
        dispatch_body,
        [sds((lines, 128), bf16), sds((seqs, part), f32)],
        mix_home,
        residual_in,
        ffn_gain,
        route_ids.T,
        scratch_shapes=[pltpu.VMEM((lines, 128), f32)],
    )
    received = lax.all_to_all(
        buffer.reshape(experts, -1, 128), ("g", "c"), 0, 0, tiled=True
    ).reshape(lines, 128)
    per_part = part // 128
    chunk = up(capacity * per_part, 8)
    targets = experts * tp_count
    sent = targets * chunk + 8 * per_part
    down = call(
        functools.partial(expert_body, capacity),
        sds((targets, chunk, 128), bf16),
        received,
        expert_gate,
        expert_up,
        expert_down,
        scratch_shapes=[
            pltpu.VMEM((lines + 8 * width // 128, 128), f32),
            pltpu.VMEM((sent, 128), f32),
        ],
    )
    back = lax.all_to_all(down, ("g", "c", "tp"), 0, 0, tiled=True)
    layer_out = call(
        combine_body,
        sds((seqs, part), bf16),
        back,
        route_ids.T,
        route_weight.T,
        own_mix,
        scratch_shapes=[pltpu.VMEM((sent, 128), f32)],
    )
    return layer_out, new_state


def solution(mesh):
    ep, tp = mesh.shape["ep"], mesh.shape["tp"]
    split = Mesh(mesh.devices.reshape(ep // 2, 2, tp), ("g", "c", "tp"))
    seq = ("g", "c")
    in_specs = (
        P(seq, None),
        P(seq, "tp", None, None),
        P(),
        P("tp", seq),
        P("tp", seq),
        P("tp", seq),
        P("tp", seq),
        P("tp"),
        P(),
        P("tp", seq),
        P(),
        P(seq, None),
        P(seq, None),
        P(seq, None, "tp"),
        P(seq, None, "tp"),
        P(seq, "tp", None),
    )
    out_specs = (P(seq, "tp"), P(seq, "tp", None, None))
    return jax.shard_map(
        shards, mesh=split, in_specs=in_specs, out_specs=out_specs, check_vma=False
    )
```

```python
import functools

import jax
import jax.numpy as jnp
from jax import lax
from jax.experimental import pallas as pl
from jax.experimental.pallas import tpu as pltpu
from jax.sharding import Mesh, PartitionSpec as P


rms_eps = 1e-06
bf16, f32 = jnp.bfloat16, jnp.float32


def dot(a, b):
    return jnp.dot(a, b, preferred_element_type=f32)


def rms_scale(values, gain):
    return values * lax.rsqrt(jnp.mean(values * values, axis=-1, keepdims=True) + rms_eps) * gain


def up(n, m):
    return -(-n // m) * m


def call(body, out_shape, *args, mib=16, cost=None, **kw):
    return pl.pallas_call(
        body,
        out_shape=out_shape,
        compiler_params=pltpu.CompilerParams(vmem_limit_bytes=mib << 20),
        cost_estimate=cost,
        **kw,
    )(*args)


def dot_t(a, b):
    return lax.dot_general(a, b, (((1,), (1,)), ((), ())), preferred_element_type=f32)


def pick_part(rank, full, part):
    own = full[:, :part]
    for t in range(1, full.shape[1] // part):
        own = jnp.where(rank == t, full[:, t * part : (t + 1) * part], own)
    return own


def core_order(core, own, other):
    return jnp.where(core == 0, own, other), jnp.where(core == 0, other, own)


def norm_body(*refs):
    sources, (out_ref, own_ref, mix_ref, res_ref, gain_ref, sems) = refs[:7], refs[7:]
    targets = [res_ref, gain_ref] + [own_ref.at[p] for p in range(4)] + [mix_ref]
    loads = [
        pltpu.make_async_copy(source, target, sems.at[i])
        for i, (source, target) in enumerate(zip(sources, targets))
    ]
    for load in loads:
        load.start()
    groups, rows, part = out_ref.shape
    tp_rank = lax.axis_index("tp")
    for load in loads[:2]:
        load.wait()
    res = res_ref[...].astype(f32)
    scale = lax.rsqrt(jnp.mean(res * res, axis=-1, keepdims=True) + rms_eps)
    normed = (res * scale * gain_ref[...].reshape(1, -1)).astype(bf16)
    half = pick_part(tp_rank, normed, part)
    half = jnp.concatenate([half, jnp.zeros((rows - half.shape[0], part), bf16)], axis=0)
    for g in range(groups):
        out_ref[g] = half
    for load in loads[2:]:
        load.wait()


def proj_body(x_ref, own_ref, oth_ref, out_ref):
    groups, rows, part = x_ref.shape
    half = out_ref.shape[-1] // 2
    x = x_ref[...].reshape(groups * rows, part)
    for i, w_ref in enumerate((own_ref, oth_ref)):
        columns = jnp.concatenate([w_ref[p] for p in range(4)], axis=0)
        y = dot_t(x, columns).astype(bf16).reshape(groups, rows, half)
        for t in range(out_ref.shape[1]):
            out_ref[:, t, :, i * half : (i + 1) * half] = y


def pack_body(own_ref, far_ref, out_ref):
    high = lax.axis_index("a") // 2
    out_ref[high] = own_ref[...]
    out_ref[1 - high] = far_ref[...]


def read_body(recv_ref, lower_ref, gain_ref, state_ref, out_ref, forget_ref, value_ref):
    groups, tp_count, rows, both = recv_ref.shape
    seqs, heads, size, _ = state_ref.shape
    pieces = groups // tp_count
    first = lax.axis_index("tp") * pieces
    core = lax.axis_index("c")
    blocks = [recv_ref[first + g].astype(f32).sum(axis=0) for g in range(pieces)]
    cols = both // 8
    proj = []
    for p in range(4):
        parts = []
        for block in blocks:
            own = block[:, p * cols : (p + 1) * cols]
            other = block[:, both // 2 + p * cols : both // 2 + (p + 1) * cols]
            parts += core_order(core, own, other)
        proj.append(jnp.concatenate(parts, axis=1).astype(bf16).astype(f32))
    query = jax.nn.silu(proj[0])
    lower = lower_ref[...].reshape(1, -1)
    forget = lower + (1.0 - lower) * jax.nn.sigmoid(proj[1])
    forget_ref[...] = forget
    value_ref[...] = proj[2]
    gate = jax.nn.silu(proj[3])
    gain = gain_ref[...].reshape(1, -1)
    mixed = query * forget
    high = mixed.astype(bf16)
    low = (mixed - high.astype(f32)).astype(bf16)
    direct = query * (1.0 - forget)
    row_ids = lax.broadcasted_iota(jnp.int32, (rows, size), 0)
    for h in range(heads):
        lanes = slice(h * size, (h + 1) * size)
        lhs = jnp.concatenate([high[:, lanes], low[:, lanes]], axis=0)
        readout = jnp.sum(direct[:, lanes], axis=1, keepdims=True) * proj[2][:, lanes]
        for s in range(seqs):
            both_parts = dot(lhs, state_ref[s, h])
            readout += jnp.where(row_ids == s, both_parts[:rows] + both_parts[rows:], 0.0)
        heads_out = (rms_scale(readout, gain) * gate[:, lanes]).astype(bf16)
        for g in range(out_ref.shape[0]):
            out_ref[g, :, lanes] = heads_out


def state_body(forget_ref, value_ref, state_ref, new_ref):
    seqs = state_ref.shape[0]
    forget_t = forget_ref[...].T
    key_t = 1.0 - forget_t
    value = value_ref[...]
    for s in range(seqs):
        new_ref[s, 0] = (
            forget_t[:, s : s + 1] * state_ref[s, 0].astype(f32)
            + key_t[:, s : s + 1] * value[s : s + 1]
        ).astype(bf16)


def mix_body(x_ref, *refs):
    *w_refs, out_ref = refs
    blocks, rows, part = x_ref.shape
    x = x_ref[...].reshape(blocks * rows, part)
    ys = [dot_t(x, w_ref[...].reshape(-1, part)) for w_ref in w_refs]
    if len(ys) == 2:
        cols = ys[0].shape[1] // 2
        low = lax.rem(lax.axis_index("a"), 2)
        ys = [
            y
            for high in range(2)
            for y in core_order(low, *(y[:, high * cols : (high + 1) * cols] for y in ys))
        ]
    y = jnp.concatenate(ys, axis=1).astype(bf16).reshape(blocks, rows, -1)
    for t in range(out_ref.shape[1]):
        out_ref[:, t] = y


def slots_of(ids, slots, experts):
    tops, seqs = ids.shape
    row = lax.broadcasted_iota(jnp.int32, (experts * slots, seqs), 0)
    expert, place = row // slots, row % slots
    named = [ids[k : k + 1] == expert for k in range(tops)]
    names = sum(n.astype(f32) for n in named)
    before = (
        lax.broadcasted_iota(jnp.int32, (seqs, seqs), 0)
        < lax.broadcasted_iota(jnp.int32, (seqs, seqs), 1)
    ).astype(f32)
    rank = dot(names.astype(bf16), before.astype(bf16))
    here = jnp.where(rank == place.astype(f32), names, 0.0)
    return here, named


def dispatch_body(recv_ref, res_ref, gain_ref, ids_ref, out_ref, own_ref, lines):
    blocks = recv_ref.shape[0]
    deep = lax.axis_size("a")
    cols = recv_ref.shape[3] // deep
    seqs, width = res_ref.shape
    per_row = width // 128
    slots_all = out_ref.shape[0] // per_row
    experts = deep * blocks
    sums = [recv_ref[g].astype(f32).sum(axis=0) for g in range(blocks)]
    mixed = jnp.concatenate(
        [x[:, a * cols : (a + 1) * cols] for a in range(deep) for x in sums], axis=1
    )[:seqs]
    after = (res_ref[...].astype(f32) + mixed).astype(bf16).astype(f32)
    normed = rms_scale(after, gain_ref[...].reshape(1, -1)).astype(bf16)
    here, _ = slots_of(ids_ref[...], slots_all // experts, experts)
    picked = dot(here.astype(bf16), normed)
    for j in range(per_row):
        lines[pl.ds(j, slots_all, stride=per_row), :] = picked[:, j * 128 : (j + 1) * 128]
    out_ref[...] = lines[...].astype(bf16)
    own_ref[...] = pick_part(lax.axis_index("tp"), after, own_ref.shape[1])


def expert_body(capacity, x_ref, gate_ref, up_ref, down_ref, out_ref, lines, sent):
    width = gate_ref.shape[1]
    per_row = width // 128
    count = x_ref.shape[0]
    sources = count // (capacity * per_row)
    lines[:count] = x_ref[...].astype(f32)
    lines[count:] = jnp.zeros((lines.shape[0] - count, 128), f32)
    x = jnp.concatenate(
        [
            jnp.concatenate(
                [
                    lines[pl.ds(e * capacity * per_row + j, 8, stride=per_row), :]
                    for j in range(per_row)
                ],
                axis=1,
            )
            for e in range(sources)
        ],
        axis=0,
    ).astype(bf16)
    hidden = (jax.nn.silu(dot(x, gate_ref[0])) * dot(x, up_ref[0])).astype(bf16)
    y = dot(hidden, down_ref[0])
    targets, chunk, _ = out_ref.shape
    tp_count = targets // sources
    per_part = per_row // tp_count
    for d in range(targets):
        e, t = d // tp_count, d % tp_count
        for j in range(per_part):
            lane = (t * per_part + j) * 128
            sent[pl.ds(d * chunk + j, 8, stride=per_part), :] = y[
                e * 8 : (e + 1) * 8, lane : lane + 128
            ]
    for d in range(targets):
        out_ref[d] = sent[d * chunk : (d + 1) * chunk].astype(bf16)


def combine_body(back_ref, ids_ref, weight_ref, own_ref, out_ref, lines):
    targets, chunk, _ = back_ref.shape
    tp_count = lax.axis_size("tp")
    experts = targets // tp_count
    per_part = own_ref.shape[1] // 128
    for d in range(targets):
        lines[d * chunk : (d + 1) * chunk] = back_ref[d].astype(f32)
    lines[targets * chunk :] = jnp.zeros((lines.shape[0] - targets * chunk, 128), f32)

    def piece(e, j):
        return sum(
            lines[pl.ds((e * tp_count + t) * chunk + j, 8, stride=per_part), :]
            for t in range(tp_count)
        )

    rows = jnp.concatenate(
        [
            jnp.concatenate([piece(e, j) for j in range(per_part)], axis=1)
            for e in range(experts)
        ],
        axis=0,
    ).astype(bf16)
    here, named = slots_of(ids_ref[...], 8, experts)
    weight = sum(jnp.where(n, weight_ref[k : k + 1], 0.0) for k, n in enumerate(named))
    weight = weight * here
    high = weight.astype(bf16)
    low = (weight - high.astype(f32)).astype(bf16)
    total = sum(
        lax.dot_general(w, rows, (((0,), (0,)), ((), ())), preferred_element_type=f32)
        for w in (high, low)
    )
    out_ref[...] = (own_ref[...] + total).astype(bf16)


def capacity_of(seqs, tops, experts):
    return max(2, seqs * tops // experts + 1)


def shards(
    residual_in,
    rec_state,
    mix_gain,
    w_query,
    w_forget,
    w_input,
    w_gate,
    lower_bound,
    head_gain,
    w_out,
    ffn_gain,
    route_ids,
    route_weight,
    expert_gate,
    expert_up,
    expert_down,
):
    deep, wide, cores, tp_count = (lax.axis_size(a) for a in ("a", "b", "c", "tp"))
    groups, plane = deep * wide, wide * cores
    chips = ("a", "b")
    seqs, width = residual_in.shape
    part = width // tp_count
    cols = w_query.shape[1]
    _, heads, size, _ = rec_state.shape
    rows = up(seqs, 16)
    sds = jax.ShapeDtypeStruct

    sources = [residual_in, mix_gain]
    sources += [w.T for w in (w_query, w_forget, w_input, w_gate, w_out)]
    vmem, hbm = (pl.BlockSpec(memory_space=m) for m in (pltpu.VMEM, pltpu.HBM))
    spread, own_w, own_o = call(
        norm_body,
        [
            sds((groups, rows, part), bf16),
            sds((4, cols, part), bf16),
            sds((cols, part), bf16),
        ],
        *(pltpu.with_memory_space_constraint(a, pltpu.HBM) for a in sources),
        in_specs=[hbm] * 7,
        out_specs=[vmem] * 3,
        scratch_shapes=[
            pltpu.VMEM(residual_in.shape, bf16),
            pltpu.VMEM(mix_gain.shape, f32),
            pltpu.SemaphoreType.DMA((7,)),
        ],
    )
    oth_w = lax.ppermute(own_w, "c", [(i, i ^ 1) for i in range(cores)])
    if deep == 4:
        far = lax.ppermute(own_o, "a", [(i, i ^ 2) for i in range(deep)])
    gathered = lax.all_to_all(spread, chips, 0, 0, tiled=True)

    partial = call(
        proj_body,
        sds((groups, tp_count, rows, 4 * cores * cols), bf16),
        gathered,
        own_w,
        oth_w,
    )
    if deep == 4:
        packs = [call(pack_body, sds((2, cols, part), bf16), own_o, far)]
        packs.append(lax.ppermute(packs[0], "a", [(i, i ^ 1) for i in range(deep)]))
    else:
        packs = [lax.all_gather(own_o, "a", axis=0).reshape(deep * cols, part)]
    arrived = lax.all_to_all(
        partial.reshape(groups * tp_count, rows, -1), (*chips, "tp"), 0, 0, tiled=True
    ).reshape(partial.shape)

    spread_heads, forget, value = call(
        read_body,
        [
            sds((plane, rows, heads * size), bf16),
            sds((rows, heads * size), f32),
            sds((rows, heads * size), f32),
        ],
        arrived,
        lower_bound,
        head_gain,
        rec_state,
    )
    if deep == 4:
        spread_heads, packs[1] = lax.optimization_barrier((spread_heads, packs[1]))
    all_heads = lax.all_to_all(spread_heads, ("b", "c"), 0, 0, tiled=True)

    per_head = pl.BlockSpec((seqs, 1, size, size), lambda i: (0, i, 0, 0))
    head_lanes = pl.BlockSpec((rows, size), lambda i: (0, i))
    new_state = call(
        state_body,
        sds(rec_state.shape, bf16),
        forget,
        value,
        rec_state,
        grid=(heads,),
        in_specs=[head_lanes, head_lanes, per_head],
        out_specs=per_head,
        cost=pl.CostEstimate(
            flops=10**7, bytes_accessed=4 * rec_state.size, transcendentals=0
        ),
    )

    partial_mix = call(
        mix_body, sds((plane, tp_count, rows, deep * cols), bf16), all_heads, *packs
    )
    mix_home = lax.all_to_all(
        partial_mix.reshape(plane * tp_count, rows, -1), ("b", "c", "tp"), 0, 0, tiled=True
    ).reshape(partial_mix.shape)

    experts = groups * cores
    capacity = capacity_of(seqs, route_ids.shape[1], experts)
    assert capacity <= 8
    lines = experts * capacity * width // 128
    buffer, own_mix = call(
        dispatch_body,
        [sds((lines, 128), bf16), sds((seqs, part), f32)],
        mix_home,
        residual_in,
        ffn_gain,
        route_ids.T,
        scratch_shapes=[pltpu.VMEM((lines, 128), f32)],
    )
    received = lax.all_to_all(
        buffer.reshape(experts, -1, 128), (*chips, "c"), 0, 0, tiled=True
    ).reshape(lines, 128)
    per_part = part // 128
    chunk = up(capacity * per_part, 8)
    targets = experts * tp_count
    sent = targets * chunk + 8 * per_part
    down = call(
        functools.partial(expert_body, capacity),
        sds((targets, chunk, 128), bf16),
        received,
        expert_gate,
        expert_up,
        expert_down,
        scratch_shapes=[
            pltpu.VMEM((lines + 8 * width // 128, 128), f32),
            pltpu.VMEM((sent, 128), f32),
        ],
    )
    back = lax.all_to_all(down, (*chips, "c", "tp"), 0, 0, tiled=True)
    layer_out = call(
        combine_body,
        sds((seqs, part), bf16),
        back,
        route_ids.T,
        route_weight.T,
        own_mix,
        scratch_shapes=[pltpu.VMEM((sent, 128), f32)],
    )
    return layer_out, new_state


def solution(mesh):
    ep, tp = mesh.shape["ep"], mesh.shape["tp"]
    wide = 2 if ep % 4 == 0 else 1
    shape = (ep // (2 * wide), wide, 2, tp)
    split = Mesh(mesh.devices.reshape(shape), ("a", "b", "c", "tp"))
    seq = ("a", "b", "c")
    in_specs = (
        P(seq, None),
        P(seq, "tp", None, None),
        P(),
        P("tp", seq),
        P("tp", seq),
        P("tp", seq),
        P("tp", seq),
        P("tp"),
        P(),
        P("tp", seq),
        P(),
        P(seq, None),
        P(seq, None),
        P(seq, None, "tp"),
        P(seq, None, "tp"),
        P(seq, "tp", None),
    )
    out_specs = (P(seq, "tp"), P(seq, "tp", None, None))
    return jax.shard_map(
        shards, mesh=split, in_specs=in_specs, out_specs=out_specs, check_vma=False
    )
```

```python
import functools

import jax
import jax.numpy as jnp
from jax import lax
from jax.experimental import pallas as pl
from jax.experimental.pallas import tpu as pltpu
from jax.sharding import Mesh, PartitionSpec as P


rms_eps = 1e-06
bf16, f32 = jnp.bfloat16, jnp.float32


def dot(a, b):
    return jnp.dot(a, b, preferred_element_type=f32)


def rms_scale(values, gain):
    return values * lax.rsqrt(jnp.mean(values * values, axis=-1, keepdims=True) + rms_eps) * gain


def up(n, m):
    return -(-n // m) * m


def call(body, out_shape, *args, mib=16, cost=None, **kw):
    return pl.pallas_call(
        body,
        out_shape=out_shape,
        compiler_params=pltpu.CompilerParams(vmem_limit_bytes=mib << 20),
        cost_estimate=cost,
        **kw,
    )(*args)


def dot_t(a, b):
    return lax.dot_general(a, b, (((1,), (1,)), ((), ())), preferred_element_type=f32)


def pick_part(rank, full, part):
    own = full[:, :part]
    for t in range(1, full.shape[1] // part):
        own = jnp.where(rank == t, full[:, t * part : (t + 1) * part], own)
    return own


def core_order(core, own, other):
    return jnp.where(core == 0, own, other), jnp.where(core == 0, other, own)


def norm_body(*refs):
    sources, (out_ref, own_ref, mix_ref, res_ref, gain_ref, sems) = refs[:7], refs[7:]
    targets = [res_ref, gain_ref] + [own_ref.at[p] for p in range(4)] + [mix_ref]
    loads = [
        pltpu.make_async_copy(source, target, sems.at[i])
        for i, (source, target) in enumerate(zip(sources, targets))
    ]
    for load in loads:
        load.start()
    groups, rows, part = out_ref.shape
    tp_rank = lax.axis_index("tp")
    for load in loads[:2]:
        load.wait()
    res = res_ref[...].astype(f32)
    scale = lax.rsqrt(jnp.mean(res * res, axis=-1, keepdims=True) + rms_eps)
    normed = (res * scale * gain_ref[...].reshape(1, -1)).astype(bf16)
    half = pick_part(tp_rank, normed, part)
    half = jnp.concatenate([half, jnp.zeros((rows - half.shape[0], part), bf16)], axis=0)
    for g in range(groups):
        out_ref[g] = half
    for load in loads[2:]:
        load.wait()


def proj_body(x_ref, own_ref, oth_ref, out_ref):
    groups, rows, part = x_ref.shape
    half = out_ref.shape[-1] // 2
    x = x_ref[...].reshape(groups * rows, part)
    for i, w_ref in enumerate((own_ref, oth_ref)):
        columns = jnp.concatenate([w_ref[p] for p in range(4)], axis=0)
        y = dot_t(x, columns).astype(bf16).reshape(groups, rows, half)
        for t in range(out_ref.shape[1]):
            out_ref[:, t, :, i * half : (i + 1) * half] = y


def pack_body(own_ref, far_ref, out_ref):
    high = lax.axis_index("a") // 2
    out_ref[high] = own_ref[...]
    out_ref[1 - high] = far_ref[...]


def read_body(recv_ref, lower_ref, gain_ref, state_ref, out_ref, forget_ref, value_ref):
    groups, tp_count, rows, both = recv_ref.shape
    seqs, heads, size, _ = state_ref.shape
    pieces = groups // tp_count
    first = lax.axis_index("tp") * pieces
    core = lax.axis_index("c")
    blocks = [recv_ref[first + g].astype(f32).sum(axis=0) for g in range(pieces)]
    cols = both // 8
    proj = []
    for p in range(4):
        parts = []
        for block in blocks:
            own = block[:, p * cols : (p + 1) * cols]
            other = block[:, both // 2 + p * cols : both // 2 + (p + 1) * cols]
            parts += core_order(core, own, other)
        proj.append(jnp.concatenate(parts, axis=1).astype(bf16).astype(f32))
    query = jax.nn.silu(proj[0])
    lower = lower_ref[...].reshape(1, -1)
    forget = lower + (1.0 - lower) * jax.nn.sigmoid(proj[1])
    forget_ref[...] = forget
    value_ref[...] = proj[2]
    gate = jax.nn.silu(proj[3])
    gain = gain_ref[...].reshape(1, -1)
    mixed = query * forget
    high = mixed.astype(bf16)
    low = (mixed - high.astype(f32)).astype(bf16)
    direct = query * (1.0 - forget)
    row_ids = lax.broadcasted_iota(jnp.int32, (rows, size), 0)
    for h in range(heads):
        lanes = slice(h * size, (h + 1) * size)
        lhs = jnp.concatenate([high[:, lanes], low[:, lanes]], axis=0)
        readout = jnp.sum(direct[:, lanes], axis=1, keepdims=True) * proj[2][:, lanes]
        for s in range(seqs):
            both_parts = dot(lhs, state_ref[s, h])
            readout += jnp.where(row_ids == s, both_parts[:rows] + both_parts[rows:], 0.0)
        heads_out = (rms_scale(readout, gain) * gate[:, lanes]).astype(bf16)
        out_ref[:, lanes] = heads_out


def state_body(forget_ref, value_ref, state_ref, new_ref):
    seqs = state_ref.shape[0]
    forget_t = forget_ref[...].T
    key_t = 1.0 - forget_t
    value = value_ref[...]
    for s in range(seqs):
        new_ref[s, 0] = (
            forget_t[:, s : s + 1] * state_ref[s, 0].astype(f32)
            + key_t[:, s : s + 1] * value[s : s + 1]
        ).astype(bf16)


def mix_body(blocks, *refs):
    x_refs, w_refs, out_ref = refs[:blocks], refs[blocks:-1], refs[-1]
    rows, part = x_refs[0].shape
    x = jnp.concatenate([x_ref[...] for x_ref in x_refs], axis=0)
    ys = [dot_t(x, w_ref[...].reshape(-1, part)) for w_ref in w_refs]
    if len(ys) == 4:
        cols = ys[0].shape[1] // 2
        low, core = lax.rem(lax.axis_index("a"), 2), lax.axis_index("c")
        own, near = core_order(core, *ys[:2]), core_order(core, *ys[2:])
        ys = []
        for high in range(2):
            lanes = slice(high * cols, (high + 1) * cols)
            pairs = [core_order(low, own[c][:, lanes], near[c][:, lanes]) for c in range(2)]
            ys += [pairs[c][a] for a in range(2) for c in range(2)]
    y = jnp.concatenate(ys, axis=1).astype(bf16)
    for i in range(blocks):
        place = lax.rem(lax.axis_index("b") + i, blocks)
        for t in range(out_ref.shape[1]):
            out_ref[place, t] = y[i * rows : (i + 1) * rows]


def slots_of(ids, slots, experts):
    tops, seqs = ids.shape
    row = lax.broadcasted_iota(jnp.int32, (experts * slots, seqs), 0)
    expert, place = row // slots, row % slots
    named = [ids[k : k + 1] == expert for k in range(tops)]
    names = sum(n.astype(f32) for n in named)
    before = (
        lax.broadcasted_iota(jnp.int32, (seqs, seqs), 0)
        < lax.broadcasted_iota(jnp.int32, (seqs, seqs), 1)
    ).astype(f32)
    rank = dot(names.astype(bf16), before.astype(bf16))
    here = jnp.where(rank == place.astype(f32), names, 0.0)
    return here, named


def dispatch_body(recv_ref, res_ref, gain_ref, ids_ref, out_ref, own_ref, lines):
    blocks = recv_ref.shape[0]
    deep = lax.axis_size("a")
    cols = recv_ref.shape[3] // deep
    seqs, width = res_ref.shape
    per_row = width // 128
    slots_all = out_ref.shape[0] // per_row
    experts = deep * blocks * lax.axis_size("c")
    sums = [recv_ref[g].astype(f32).sum(axis=0) for g in range(blocks)]
    mixed = jnp.concatenate(
        [x[:, a * cols : (a + 1) * cols] for a in range(deep) for x in sums], axis=1
    )[:seqs]
    after = (res_ref[...].astype(f32) + mixed).astype(bf16).astype(f32)
    normed = rms_scale(after, gain_ref[...].reshape(1, -1)).astype(bf16)
    here, _ = slots_of(ids_ref[...], slots_all // experts, experts)
    picked = dot(here.astype(bf16), normed)
    for j in range(per_row):
        lines[pl.ds(j, slots_all, stride=per_row), :] = picked[:, j * 128 : (j + 1) * 128]
    out_ref[...] = lines[...].astype(bf16)
    own_ref[...] = pick_part(lax.axis_index("tp"), after, own_ref.shape[1])


def expert_body(capacity, x_ref, gate_ref, up_ref, down_ref, out_ref, lines, sent):
    width = gate_ref.shape[1]
    per_row = width // 128
    count = x_ref.shape[0]
    sources = count // (capacity * per_row)
    lines[:count] = x_ref[...].astype(f32)
    lines[count:] = jnp.zeros((lines.shape[0] - count, 128), f32)
    x = jnp.concatenate(
        [
            jnp.concatenate(
                [
                    lines[pl.ds(e * capacity * per_row + j, 8, stride=per_row), :]
                    for j in range(per_row)
                ],
                axis=1,
            )
            for e in range(sources)
        ],
        axis=0,
    ).astype(bf16)
    hidden = (jax.nn.silu(dot(x, gate_ref[0])) * dot(x, up_ref[0])).astype(bf16)
    y = dot(hidden, down_ref[0])
    targets, chunk, _ = out_ref.shape
    tp_count = targets // sources
    per_part = per_row // tp_count
    for d in range(targets):
        e, t = d // tp_count, d % tp_count
        for j in range(per_part):
            lane = (t * per_part + j) * 128
            sent[pl.ds(d * chunk + j, 8, stride=per_part), :] = y[
                e * 8 : (e + 1) * 8, lane : lane + 128
            ]
    for d in range(targets):
        out_ref[d] = sent[d * chunk : (d + 1) * chunk].astype(bf16)


def combine_body(back_ref, ids_ref, weight_ref, own_ref, out_ref, lines):
    targets, chunk, _ = back_ref.shape
    tp_count = lax.axis_size("tp")
    experts = targets // tp_count
    per_part = own_ref.shape[1] // 128
    for d in range(targets):
        lines[d * chunk : (d + 1) * chunk] = back_ref[d].astype(f32)
    lines[targets * chunk :] = jnp.zeros((lines.shape[0] - targets * chunk, 128), f32)

    def piece(e, j):
        return sum(
            lines[pl.ds((e * tp_count + t) * chunk + j, 8, stride=per_part), :]
            for t in range(tp_count)
        )

    rows = jnp.concatenate(
        [
            jnp.concatenate([piece(e, j) for j in range(per_part)], axis=1)
            for e in range(experts)
        ],
        axis=0,
    ).astype(bf16)
    here, named = slots_of(ids_ref[...], 8, experts)
    weight = sum(jnp.where(n, weight_ref[k : k + 1], 0.0) for k, n in enumerate(named))
    weight = weight * here
    high = weight.astype(bf16)
    low = (weight - high.astype(f32)).astype(bf16)
    total = sum(
        lax.dot_general(w, rows, (((0,), (0,)), ((), ())), preferred_element_type=f32)
        for w in (high, low)
    )
    out_ref[...] = (own_ref[...] + total).astype(bf16)


def capacity_of(seqs, tops, experts):
    return max(2, seqs * tops // experts + 1)


def shards(
    residual_in,
    rec_state,
    mix_gain,
    w_query,
    w_forget,
    w_input,
    w_gate,
    lower_bound,
    head_gain,
    w_out,
    ffn_gain,
    route_ids,
    route_weight,
    expert_gate,
    expert_up,
    expert_down,
):
    deep, wide, cores, tp_count = (lax.axis_size(a) for a in ("a", "b", "c", "tp"))
    groups = deep * wide
    chips = ("a", "b")
    seqs, width = residual_in.shape
    part = width // tp_count
    cols = w_query.shape[1]
    _, heads, size, _ = rec_state.shape
    rows = up(seqs, 16)
    sds = jax.ShapeDtypeStruct

    sources = [residual_in, mix_gain]
    sources += [w.T for w in (w_query, w_forget, w_input, w_gate, w_out)]
    vmem, hbm = (pl.BlockSpec(memory_space=m) for m in (pltpu.VMEM, pltpu.HBM))
    spread, own_w, own_o = call(
        norm_body,
        [
            sds((groups, rows, part), bf16),
            sds((4, cols, part), bf16),
            sds((cols, part), bf16),
        ],
        *(pltpu.with_memory_space_constraint(a, pltpu.HBM) for a in sources),
        in_specs=[hbm] * 7,
        out_specs=[vmem] * 3,
        scratch_shapes=[
            pltpu.VMEM(residual_in.shape, bf16),
            pltpu.VMEM(mix_gain.shape, f32),
            pltpu.SemaphoreType.DMA((7,)),
        ],
    )
    swap = [(i, i ^ 1) for i in range(cores)]
    oth_w = lax.ppermute(own_w, "c", swap)
    if deep == 4:
        far = lax.ppermute(own_o, "a", [(i, i ^ 2) for i in range(deep)])
    gathered = lax.all_to_all(spread, chips, 0, 0, tiled=True)

    partial = call(
        proj_body,
        sds((groups, tp_count, rows, 4 * cores * cols), bf16),
        gathered,
        own_w,
        oth_w,
    )
    if deep == 4:
        packs = [call(pack_body, sds((2, cols, part), bf16), own_o, far)]
        near = lax.ppermute(packs[0], "a", [(i, i ^ 1) for i in range(deep)])
        packs.append(lax.ppermute(packs[0], "c", swap))
        packs += [near, lax.ppermute(near, "c", swap)]
    else:
        packs = [lax.all_gather(own_o, ("a", "c"), axis=0).reshape(-1, part)]
    arrived = lax.all_to_all(
        partial.reshape(groups * tp_count, rows, -1), (*chips, "tp"), 0, 0, tiled=True
    ).reshape(partial.shape)

    own_heads, forget, value = call(
        read_body,
        [
            sds((rows, heads * size), bf16),
            sds((rows, heads * size), f32),
            sds((rows, heads * size), f32),
        ],
        arrived,
        lower_bound,
        head_gain,
        rec_state,
    )
    all_heads = [own_heads] + [
        lax.ppermute(own_heads, "b", [(i, (i + s) % wide) for i in range(wide)])
        for s in range(1, wide)
    ]

    per_head = pl.BlockSpec((seqs, 1, size, size), lambda i: (0, i, 0, 0))
    head_lanes = pl.BlockSpec((rows, size), lambda i: (0, i))
    new_state = call(
        state_body,
        sds(rec_state.shape, bf16),
        forget,
        value,
        rec_state,
        grid=(heads,),
        in_specs=[head_lanes, head_lanes, per_head],
        out_specs=per_head,
        cost=pl.CostEstimate(
            flops=10**7, bytes_accessed=4 * rec_state.size, transcendentals=0
        ),
    )

    partial_mix = call(
        functools.partial(mix_body, wide),
        sds((wide, tp_count, rows, deep * cores * cols), bf16),
        *all_heads,
        *packs,
    )
    mix_home = lax.all_to_all(
        partial_mix.reshape(wide * tp_count, rows, -1), ("b", "tp"), 0, 0, tiled=True
    ).reshape(partial_mix.shape)

    experts = groups * cores
    capacity = capacity_of(seqs, route_ids.shape[1], experts)
    assert capacity <= 8
    lines = experts * capacity * width // 128
    buffer, own_mix = call(
        dispatch_body,
        [sds((lines, 128), bf16), sds((seqs, part), f32)],
        mix_home,
        residual_in,
        ffn_gain,
        route_ids.T,
        scratch_shapes=[pltpu.VMEM((lines, 128), f32)],
    )
    received = lax.all_to_all(
        buffer.reshape(experts, -1, 128), (*chips, "c"), 0, 0, tiled=True
    ).reshape(lines, 128)
    per_part = part // 128
    chunk = up(capacity * per_part, 8)
    targets = experts * tp_count
    sent = targets * chunk + 8 * per_part
    down = call(
        functools.partial(expert_body, capacity),
        sds((targets, chunk, 128), bf16),
        received,
        expert_gate,
        expert_up,
        expert_down,
        scratch_shapes=[
            pltpu.VMEM((lines + 8 * width // 128, 128), f32),
            pltpu.VMEM((sent, 128), f32),
        ],
    )
    back = lax.all_to_all(down, (*chips, "c", "tp"), 0, 0, tiled=True)
    layer_out = call(
        combine_body,
        sds((seqs, part), bf16),
        back,
        route_ids.T,
        route_weight.T,
        own_mix,
        scratch_shapes=[pltpu.VMEM((sent, 128), f32)],
    )
    return layer_out, new_state


def solution(mesh):
    ep, tp = mesh.shape["ep"], mesh.shape["tp"]
    wide = 2 if ep % 4 == 0 else 1
    shape = (ep // (2 * wide), wide, 2, tp)
    split = Mesh(mesh.devices.reshape(shape), ("a", "b", "c", "tp"))
    seq = ("a", "b", "c")
    in_specs = (
        P(seq, None),
        P(seq, "tp", None, None),
        P(),
        P("tp", seq),
        P("tp", seq),
        P("tp", seq),
        P("tp", seq),
        P("tp"),
        P(),
        P("tp", seq),
        P(),
        P(seq, None),
        P(seq, None),
        P(seq, None, "tp"),
        P(seq, None, "tp"),
        P(seq, "tp", None),
    )
    out_specs = (P(seq, "tp"), P(seq, "tp", None, None))
    return jax.shard_map(
        shards, mesh=split, in_specs=in_specs, out_specs=out_specs, check_vma=False
    )
```

```python
import functools

import jax
import jax.numpy as jnp
from jax import lax
from jax.experimental import pallas as pl
from jax.experimental.pallas import tpu as pltpu
from jax.sharding import Mesh, PartitionSpec as P


rms_eps = 1e-06
bf16, f32 = jnp.bfloat16, jnp.float32


def dot(a, b):
    return jnp.dot(a, b, preferred_element_type=f32)


def rms_scale(values, gain):
    return values * lax.rsqrt(jnp.mean(values * values, axis=-1, keepdims=True) + rms_eps) * gain


def up(n, m):
    return -(-n // m) * m


def call(body, out_shape, *args, mib=16, cost=None, **kw):
    return pl.pallas_call(
        body,
        out_shape=out_shape,
        compiler_params=pltpu.CompilerParams(vmem_limit_bytes=mib << 20),
        cost_estimate=cost,
        **kw,
    )(*args)


def dot_t(a, b):
    return lax.dot_general(a, b, (((1,), (1,)), ((), ())), preferred_element_type=f32)


def pick_part(rank, full, part):
    own = full[:, :part]
    for t in range(1, full.shape[1] // part):
        own = jnp.where(rank == t, full[:, t * part : (t + 1) * part], own)
    return own


def core_order(core, own, other):
    return jnp.where(core == 0, own, other), jnp.where(core == 0, other, own)


def norm_body(*refs):
    sources, (out_ref, own_ref, mix_ref, res_ref, gain_ref, sems) = refs[:7], refs[7:]
    targets = [res_ref, gain_ref] + [own_ref.at[p] for p in range(4)] + [mix_ref]
    loads = [
        pltpu.make_async_copy(source, target, sems.at[i])
        for i, (source, target) in enumerate(zip(sources, targets))
    ]
    for load in loads:
        load.start()
    groups, rows, part = out_ref.shape
    tp_rank = lax.axis_index("tp")
    for load in loads[:2]:
        load.wait()
    res = res_ref[...].astype(f32)
    scale = lax.rsqrt(jnp.mean(res * res, axis=-1, keepdims=True) + rms_eps)
    normed = (res * scale * gain_ref[...].reshape(1, -1)).astype(bf16)
    half = pick_part(tp_rank, normed, part)
    half = jnp.concatenate([half, jnp.zeros((rows - half.shape[0], part), bf16)], axis=0)
    for g in range(groups):
        out_ref[g] = half
    for load in loads[2:]:
        load.wait()


def proj_body(x_ref, own_ref, oth_ref, out_ref):
    groups, rows, part = x_ref.shape
    half = out_ref.shape[-1] // 2
    x = x_ref[...].reshape(groups * rows, part)
    for i, w_ref in enumerate((own_ref, oth_ref)):
        columns = jnp.concatenate([w_ref[p] for p in range(4)], axis=0)
        y = dot_t(x, columns).astype(bf16).reshape(groups, rows, half)
        for t in range(out_ref.shape[1]):
            out_ref[:, t, :, i * half : (i + 1) * half] = y


def pack_body(own_ref, far_ref, out_ref):
    high = lax.axis_index("a") // 2
    out_ref[high] = own_ref[...]
    out_ref[1 - high] = far_ref[...]


def read_body(recv_ref, lower_ref, gain_ref, state_ref, out_ref, forget_ref, value_ref):
    groups, tp_count, rows, both = recv_ref.shape
    seqs, heads, size, _ = state_ref.shape
    pieces = groups // tp_count
    first = lax.axis_index("tp") * pieces
    core = lax.axis_index("c")
    blocks = [recv_ref[first + g].astype(f32).sum(axis=0) for g in range(pieces)]
    cols = both // 8
    proj = []
    for p in range(4):
        parts = []
        for block in blocks:
            own = block[:, p * cols : (p + 1) * cols]
            other = block[:, both // 2 + p * cols : both // 2 + (p + 1) * cols]
            parts += core_order(core, own, other)
        proj.append(jnp.concatenate(parts, axis=1).astype(bf16).astype(f32))
    query = jax.nn.silu(proj[0])
    lower = lower_ref[...].reshape(1, -1)
    forget = lower + (1.0 - lower) * jax.nn.sigmoid(proj[1])
    forget_ref[...] = forget
    value_ref[...] = proj[2]
    gate = jax.nn.silu(proj[3])
    gain = gain_ref[...].reshape(1, -1)
    mixed = query * forget
    high = mixed.astype(bf16)
    low = (mixed - high.astype(f32)).astype(bf16)
    direct = query * (1.0 - forget)
    row_ids = lax.broadcasted_iota(jnp.int32, (rows, size), 0)
    for h in range(heads):
        lanes = slice(h * size, (h + 1) * size)
        lhs = jnp.concatenate([high[:, lanes], low[:, lanes]], axis=0)
        readout = jnp.sum(direct[:, lanes], axis=1, keepdims=True) * proj[2][:, lanes]
        for s in range(seqs):
            both_parts = dot(lhs, state_ref[s, h])
            readout += jnp.where(row_ids == s, both_parts[:rows] + both_parts[rows:], 0.0)
        heads_out = (rms_scale(readout, gain) * gate[:, lanes]).astype(bf16)
        out_ref[:, lanes] = heads_out


def state_body(forget_ref, value_ref, state_ref, new_ref):
    seqs = state_ref.shape[0]
    forget_t = forget_ref[...].T
    key_t = 1.0 - forget_t
    value = value_ref[...]
    for s in range(seqs):
        new_ref[s, 0] = (
            forget_t[:, s : s + 1] * state_ref[s, 0].astype(f32)
            + key_t[:, s : s + 1] * value[s : s + 1]
        ).astype(bf16)


def mix_body(blocks, *refs):
    x_refs, w_refs, out_refs = refs[:blocks], refs[blocks:-blocks], refs[-blocks:]
    rows, part = x_refs[0].shape
    x = jnp.concatenate([x_ref[...] for x_ref in x_refs], axis=0)
    ys = [dot_t(x, w_ref[...].reshape(-1, part)) for w_ref in w_refs]
    if len(ys) == 4:
        cols = ys[0].shape[1] // 2
        low, core = lax.rem(lax.axis_index("a"), 2), lax.axis_index("c")
        own, near = core_order(core, *ys[:2]), core_order(core, *ys[2:])
        ys = []
        for high in range(2):
            lanes = slice(high * cols, (high + 1) * cols)
            pairs = [core_order(low, own[c][:, lanes], near[c][:, lanes]) for c in range(2)]
            ys += [pairs[c][a] for a in range(2) for c in range(2)]
    y = jnp.concatenate(ys, axis=1).astype(bf16)
    for i, out_ref in enumerate(out_refs):
        out_ref[...] = y[i * rows : (i + 1) * rows]


def slots_of(ids, slots, experts):
    tops, seqs = ids.shape
    row = lax.broadcasted_iota(jnp.int32, (experts * slots, seqs), 0)
    expert, place = row // slots, row % slots
    named = [ids[k : k + 1] == expert for k in range(tops)]
    names = sum(n.astype(f32) for n in named)
    before = (
        lax.broadcasted_iota(jnp.int32, (seqs, seqs), 0)
        < lax.broadcasted_iota(jnp.int32, (seqs, seqs), 1)
    ).astype(f32)
    rank = dot(names.astype(bf16), before.astype(bf16))
    here = jnp.where(rank == place.astype(f32), names, 0.0)
    return here, named


def dispatch_body(blocks, *refs):
    recv_refs, (res_ref, gain_ref, ids_ref, out_ref, own_ref, lines) = refs[:-6], refs[-6:]
    deep = lax.axis_size("a")
    cols = recv_refs[0].shape[1] // deep
    seqs, width = res_ref.shape
    per_row = width // 128
    slots_all = out_ref.shape[0] // per_row
    experts = deep * blocks * lax.axis_size("c")
    each = len(recv_refs) // blocks
    sums = [
        sum(r[...].astype(f32) for r in recv_refs[g * each : (g + 1) * each])
        for g in range(blocks)
    ]
    if blocks == 2:
        sums = core_order(lax.axis_index("b"), *sums)
    mixed = jnp.concatenate(
        [x[:, a * cols : (a + 1) * cols] for a in range(deep) for x in sums], axis=1
    )[:seqs]
    after = (res_ref[...].astype(f32) + mixed).astype(bf16).astype(f32)
    normed = rms_scale(after, gain_ref[...].reshape(1, -1)).astype(bf16)
    here, _ = slots_of(ids_ref[...], slots_all // experts, experts)
    picked = dot(here.astype(bf16), normed)
    for j in range(per_row):
        lines[pl.ds(j, slots_all, stride=per_row), :] = picked[:, j * 128 : (j + 1) * 128]
    out_ref[...] = lines[...].astype(bf16)
    own_ref[...] = pick_part(lax.axis_index("tp"), after, own_ref.shape[1])


def expert_body(capacity, x_ref, gate_ref, up_ref, down_ref, out_ref, lines, sent):
    width = gate_ref.shape[1]
    per_row = width // 128
    count = x_ref.shape[0]
    sources = count // (capacity * per_row)
    lines[:count] = x_ref[...].astype(f32)
    lines[count:] = jnp.zeros((lines.shape[0] - count, 128), f32)
    x = jnp.concatenate(
        [
            jnp.concatenate(
                [
                    lines[pl.ds(e * capacity * per_row + j, 8, stride=per_row), :]
                    for j in range(per_row)
                ],
                axis=1,
            )
            for e in range(sources)
        ],
        axis=0,
    ).astype(bf16)
    hidden = (jax.nn.silu(dot(x, gate_ref[0])) * dot(x, up_ref[0])).astype(bf16)
    y = dot(hidden, down_ref[0])
    targets, chunk, _ = out_ref.shape
    tp_count = targets // sources
    per_part = per_row // tp_count
    for d in range(targets):
        e, t = d // tp_count, d % tp_count
        for j in range(per_part):
            lane = (t * per_part + j) * 128
            sent[pl.ds(d * chunk + j, 8, stride=per_part), :] = y[
                e * 8 : (e + 1) * 8, lane : lane + 128
            ]
    for d in range(targets):
        out_ref[d] = sent[d * chunk : (d + 1) * chunk].astype(bf16)


def combine_body(back_ref, ids_ref, weight_ref, own_ref, out_ref, lines):
    targets, chunk, _ = back_ref.shape
    tp_count = lax.axis_size("tp")
    experts = targets // tp_count
    per_part = own_ref.shape[1] // 128
    for d in range(targets):
        lines[d * chunk : (d + 1) * chunk] = back_ref[d].astype(f32)
    lines[targets * chunk :] = jnp.zeros((lines.shape[0] - targets * chunk, 128), f32)

    def piece(e, j):
        return sum(
            lines[pl.ds((e * tp_count + t) * chunk + j, 8, stride=per_part), :]
            for t in range(tp_count)
        )

    rows = jnp.concatenate(
        [
            jnp.concatenate([piece(e, j) for j in range(per_part)], axis=1)
            for e in range(experts)
        ],
        axis=0,
    ).astype(bf16)
    here, named = slots_of(ids_ref[...], 8, experts)
    weight = sum(jnp.where(n, weight_ref[k : k + 1], 0.0) for k, n in enumerate(named))
    weight = weight * here
    high = weight.astype(bf16)
    low = (weight - high.astype(f32)).astype(bf16)
    total = sum(
        lax.dot_general(w, rows, (((0,), (0,)), ((), ())), preferred_element_type=f32)
        for w in (high, low)
    )
    out_ref[...] = (own_ref[...] + total).astype(bf16)


def capacity_of(seqs, tops, experts):
    return max(2, seqs * tops // experts + 1)


def shards(
    residual_in,
    rec_state,
    mix_gain,
    w_query,
    w_forget,
    w_input,
    w_gate,
    lower_bound,
    head_gain,
    w_out,
    ffn_gain,
    route_ids,
    route_weight,
    expert_gate,
    expert_up,
    expert_down,
):
    deep, wide, cores, tp_count = (lax.axis_size(a) for a in ("a", "b", "c", "tp"))
    groups = deep * wide
    chips = ("a", "b")
    seqs, width = residual_in.shape
    part = width // tp_count
    cols = w_query.shape[1]
    _, heads, size, _ = rec_state.shape
    rows = up(seqs, 16)
    sds = jax.ShapeDtypeStruct

    sources = [residual_in, mix_gain]
    sources += [w.T for w in (w_query, w_forget, w_input, w_gate, w_out)]
    vmem, hbm = (pl.BlockSpec(memory_space=m) for m in (pltpu.VMEM, pltpu.HBM))
    spread, own_w, own_o = call(
        norm_body,
        [
            sds((groups, rows, part), bf16),
            sds((4, cols, part), bf16),
            sds((cols, part), bf16),
        ],
        *(pltpu.with_memory_space_constraint(a, pltpu.HBM) for a in sources),
        in_specs=[hbm] * 7,
        out_specs=[vmem] * 3,
        scratch_shapes=[
            pltpu.VMEM(residual_in.shape, bf16),
            pltpu.VMEM(mix_gain.shape, f32),
            pltpu.SemaphoreType.DMA((7,)),
        ],
    )
    swap = [(i, i ^ 1) for i in range(cores)]
    oth_w = lax.ppermute(own_w, "c", swap)
    if deep == 4:
        far = lax.ppermute(own_o, "a", [(i, i ^ 2) for i in range(deep)])
    gathered = lax.all_to_all(spread, chips, 0, 0, tiled=True)

    partial = call(
        proj_body,
        sds((groups, tp_count, rows, 4 * cores * cols), bf16),
        gathered,
        own_w,
        oth_w,
    )
    if deep == 4:
        packs = [call(pack_body, sds((2, cols, part), bf16), own_o, far)]
        near = lax.ppermute(packs[0], "a", [(i, i ^ 1) for i in range(deep)])
        packs.append(lax.ppermute(packs[0], "c", swap))
        packs += [near, lax.ppermute(near, "c", swap)]
    else:
        packs = [lax.all_gather(own_o, ("a", "c"), axis=0).reshape(-1, part)]
    arrived = lax.all_to_all(
        partial.reshape(groups * tp_count, rows, -1), (*chips, "tp"), 0, 0, tiled=True
    ).reshape(partial.shape)

    own_heads, forget, value = call(
        read_body,
        [
            sds((rows, heads * size), bf16),
            sds((rows, heads * size), f32),
            sds((rows, heads * size), f32),
        ],
        arrived,
        lower_bound,
        head_gain,
        rec_state,
    )
    all_heads = [own_heads] + [
        lax.ppermute(own_heads, "b", [(i, (i + s) % wide) for i in range(wide)])
        for s in range(1, wide)
    ]

    per_head = pl.BlockSpec((seqs, 1, size, size), lambda i: (0, i, 0, 0))
    head_lanes = pl.BlockSpec((rows, size), lambda i: (0, i))
    new_state = call(
        state_body,
        sds(rec_state.shape, bf16),
        forget,
        value,
        rec_state,
        grid=(heads,),
        in_specs=[head_lanes, head_lanes, per_head],
        out_specs=per_head,
        cost=pl.CostEstimate(
            flops=10**7, bytes_accessed=4 * rec_state.size, transcendentals=0
        ),
    )

    partial_mix = call(
        functools.partial(mix_body, wide),
        [sds((rows, deep * cores * cols), bf16)] * wide,
        *all_heads,
        *packs,
    )
    mix_home = []
    for i in range(wide):
        for t in range(tp_count):
            perm = [
                (b * tp_count + p, (b + i) % wide * tp_count + (p + t) % tp_count)
                for b in range(wide)
                for p in range(tp_count)
            ]
            moved = lax.ppermute(partial_mix[i], ("b", "tp"), perm) if i + t else partial_mix[0]
            mix_home.append(moved)

    experts = groups * cores
    capacity = capacity_of(seqs, route_ids.shape[1], experts)
    assert capacity <= 8
    lines = experts * capacity * width // 128
    buffer, own_mix = call(
        functools.partial(dispatch_body, wide),
        [sds((lines, 128), bf16), sds((seqs, part), f32)],
        *mix_home,
        residual_in,
        ffn_gain,
        route_ids.T,
        scratch_shapes=[pltpu.VMEM((lines, 128), f32)],
    )
    received = lax.all_to_all(
        buffer.reshape(experts, -1, 128), (*chips, "c"), 0, 0, tiled=True
    ).reshape(lines, 128)
    per_part = part // 128
    chunk = up(capacity * per_part, 8)
    targets = experts * tp_count
    sent = targets * chunk + 8 * per_part
    down = call(
        functools.partial(expert_body, capacity),
        sds((targets, chunk, 128), bf16),
        received,
        expert_gate,
        expert_up,
        expert_down,
        scratch_shapes=[
            pltpu.VMEM((lines + 8 * width // 128, 128), f32),
            pltpu.VMEM((sent, 128), f32),
        ],
    )
    back = lax.all_to_all(down, (*chips, "c", "tp"), 0, 0, tiled=True)
    layer_out = call(
        combine_body,
        sds((seqs, part), bf16),
        back,
        route_ids.T,
        route_weight.T,
        own_mix,
        scratch_shapes=[pltpu.VMEM((sent, 128), f32)],
    )
    return layer_out, new_state


def solution(mesh):
    ep, tp = mesh.shape["ep"], mesh.shape["tp"]
    wide = 2 if ep % 4 == 0 else 1
    shape = (ep // (2 * wide), wide, 2, tp)
    split = Mesh(mesh.devices.reshape(shape), ("a", "b", "c", "tp"))
    seq = ("a", "b", "c")
    in_specs = (
        P(seq, None),
        P(seq, "tp", None, None),
        P(),
        P("tp", seq),
        P("tp", seq),
        P("tp", seq),
        P("tp", seq),
        P("tp"),
        P(),
        P("tp", seq),
        P(),
        P(seq, None),
        P(seq, None),
        P(seq, None, "tp"),
        P(seq, None, "tp"),
        P(seq, "tp", None),
    )
    out_specs = (P(seq, "tp"), P(seq, "tp", None, None))
    return jax.shard_map(
        shards, mesh=split, in_specs=in_specs, out_specs=out_specs, check_vma=False
    )
```

```python
import functools

import jax
import jax.numpy as jnp
from jax import lax
from jax.experimental import pallas as pl
from jax.experimental.pallas import tpu as pltpu
from jax.sharding import Mesh, PartitionSpec as P


rms_eps = 1e-06
bf16, f32 = jnp.bfloat16, jnp.float32


def dot(a, b):
    return jnp.dot(a, b, preferred_element_type=f32)


def rms_scale(values, gain):
    return values * lax.rsqrt(jnp.mean(values * values, axis=-1, keepdims=True) + rms_eps) * gain


def up(n, m):
    return -(-n // m) * m


def call(body, out_shape, *args, mib=16, cost=None, **kw):
    return pl.pallas_call(
        body,
        out_shape=out_shape,
        compiler_params=pltpu.CompilerParams(vmem_limit_bytes=mib << 20),
        cost_estimate=cost,
        **kw,
    )(*args)


def dot_t(a, b):
    return lax.dot_general(a, b, (((1,), (1,)), ((), ())), preferred_element_type=f32)


def pick_part(rank, full, part):
    own = full[:, :part]
    for t in range(1, full.shape[1] // part):
        own = jnp.where(rank == t, full[:, t * part : (t + 1) * part], own)
    return own


def core_order(core, own, other):
    return jnp.where(core == 0, own, other), jnp.where(core == 0, other, own)


def norm_body(*refs):
    sources, (out_ref, own_ref, mix_ref, res_ref, gain_ref, sems) = refs[:7], refs[7:]
    targets = [res_ref, gain_ref] + [own_ref.at[p] for p in range(4)] + [mix_ref]
    loads = [
        pltpu.make_async_copy(source, target, sems.at[i])
        for i, (source, target) in enumerate(zip(sources, targets))
    ]
    for load in loads:
        load.start()
    groups, rows, part = out_ref.shape
    tp_rank = lax.axis_index("tp")
    for load in loads[:2]:
        load.wait()
    res = res_ref[...].astype(f32)
    scale = lax.rsqrt(jnp.mean(res * res, axis=-1, keepdims=True) + rms_eps)
    normed = (res * scale * gain_ref[...].reshape(1, -1)).astype(bf16)
    half = pick_part(tp_rank, normed, part)
    half = jnp.concatenate([half, jnp.zeros((rows - half.shape[0], part), bf16)], axis=0)
    for g in range(groups):
        out_ref[g] = half
    for load in loads[2:]:
        load.wait()


def proj_body(x_ref, own_ref, oth_ref, out_ref):
    groups, rows, part = x_ref.shape
    half = out_ref.shape[-1] // 2
    x = x_ref[...].reshape(groups * rows, part)
    for i, w_ref in enumerate((own_ref, oth_ref)):
        columns = jnp.concatenate([w_ref[p] for p in range(4)], axis=0)
        y = dot_t(x, columns).astype(bf16).reshape(groups, rows, half)
        for t in range(out_ref.shape[1]):
            out_ref[:, t, :, i * half : (i + 1) * half] = y


def pack_body(own_ref, far_ref, out_ref):
    high = lax.axis_index("a") // 2
    out_ref[high] = own_ref[...]
    out_ref[1 - high] = far_ref[...]


def read_body(recv_ref, lower_ref, gain_ref, state_ref, out_ref, forget_ref, value_ref):
    groups, tp_count, rows, both = recv_ref.shape
    seqs, heads, size, _ = state_ref.shape
    pieces = groups // tp_count
    first = lax.axis_index("tp") * pieces
    core = lax.axis_index("c")
    blocks = [recv_ref[first + g].astype(f32).sum(axis=0) for g in range(pieces)]
    cols = both // 8
    proj = []
    for p in range(4):
        parts = []
        for block in blocks:
            own = block[:, p * cols : (p + 1) * cols]
            other = block[:, both // 2 + p * cols : both // 2 + (p + 1) * cols]
            parts += core_order(core, own, other)
        proj.append(jnp.concatenate(parts, axis=1).astype(bf16).astype(f32))
    query = jax.nn.silu(proj[0])
    lower = lower_ref[...].reshape(1, -1)
    forget = lower + (1.0 - lower) * jax.nn.sigmoid(proj[1])
    forget_ref[...] = forget
    value_ref[...] = proj[2]
    gate = jax.nn.silu(proj[3])
    gain = gain_ref[...].reshape(1, -1)
    mixed = query * forget
    high = mixed.astype(bf16)
    low = (mixed - high.astype(f32)).astype(bf16)
    direct = query * (1.0 - forget)
    row_ids = lax.broadcasted_iota(jnp.int32, (rows, size), 0)
    for h in range(heads):
        lanes = slice(h * size, (h + 1) * size)
        lhs = jnp.concatenate([high[:, lanes], low[:, lanes]], axis=0)
        readout = jnp.sum(direct[:, lanes], axis=1, keepdims=True) * proj[2][:, lanes]
        for s in range(seqs):
            both_parts = dot(lhs, state_ref[s, h])
            readout += jnp.where(row_ids == s, both_parts[:rows] + both_parts[rows:], 0.0)
        heads_out = (rms_scale(readout, gain) * gate[:, lanes]).astype(bf16)
        out_ref[:, lanes] = heads_out


def state_body(forget_ref, value_ref, state_ref, new_ref):
    seqs = state_ref.shape[0]
    forget_t = forget_ref[...].T
    key_t = 1.0 - forget_t
    value = value_ref[...]
    for s in range(seqs):
        new_ref[s, 0] = (
            forget_t[:, s : s + 1] * state_ref[s, 0].astype(f32)
            + key_t[:, s : s + 1] * value[s : s + 1]
        ).astype(bf16)


def mix_body(blocks, *refs):
    x_refs, w_refs, out_refs = refs[:blocks], refs[blocks:-blocks], refs[-blocks:]
    rows, part = x_refs[0].shape
    x = jnp.concatenate([x_ref[...] for x_ref in x_refs], axis=0)
    ys = [dot_t(x, w_ref[...].reshape(-1, part)) for w_ref in w_refs]
    if len(ys) == 6:
        cols = ys[2].shape[1]
        high, low = lax.axis_index("a") // 2, lax.rem(lax.axis_index("a"), 2)
        own, side, past = (core_order(lax.axis_index("c"), *ys[i : i + 2]) for i in (0, 2, 4))
        near = [core_order(high, side[c], past[c]) for c in range(2)]
        ys = []
        for h in range(2):
            lanes = slice(h * cols, (h + 1) * cols)
            pairs = [core_order(low, own[c][:, lanes], near[c][h]) for c in range(2)]
            ys += [pairs[c][a] for a in range(2) for c in range(2)]
    y = jnp.concatenate(ys, axis=1).astype(bf16)
    for i, out_ref in enumerate(out_refs):
        out_ref[...] = y[i * rows : (i + 1) * rows]


def slots_of(ids, slots, experts):
    tops, seqs = ids.shape
    row = lax.broadcasted_iota(jnp.int32, (experts * slots, seqs), 0)
    expert, place = row // slots, row % slots
    named = [ids[k : k + 1] == expert for k in range(tops)]
    names = sum(n.astype(f32) for n in named)
    before = (
        lax.broadcasted_iota(jnp.int32, (seqs, seqs), 0)
        < lax.broadcasted_iota(jnp.int32, (seqs, seqs), 1)
    ).astype(f32)
    rank = dot(names.astype(bf16), before.astype(bf16))
    here = jnp.where(rank == place.astype(f32), names, 0.0)
    return here, named


def dispatch_body(blocks, *refs):
    recv_refs, (res_ref, gain_ref, ids_ref, out_ref, own_ref, lines) = refs[:-6], refs[-6:]
    deep = lax.axis_size("a")
    cols = recv_refs[0].shape[1] // deep
    seqs, width = res_ref.shape
    per_row = width // 128
    slots_all = out_ref.shape[0] // per_row
    experts = deep * blocks * lax.axis_size("c")
    each = len(recv_refs) // blocks
    sums = [
        sum(r[...].astype(f32) for r in recv_refs[g * each : (g + 1) * each])
        for g in range(blocks)
    ]
    if blocks == 2:
        sums = core_order(lax.axis_index("b"), *sums)
    mixed = jnp.concatenate(
        [x[:, a * cols : (a + 1) * cols] for a in range(deep) for x in sums], axis=1
    )[:seqs]
    after = (res_ref[...].astype(f32) + mixed).astype(bf16).astype(f32)
    normed = rms_scale(after, gain_ref[...].reshape(1, -1)).astype(bf16)
    here, _ = slots_of(ids_ref[...], slots_all // experts, experts)
    picked = dot(here.astype(bf16), normed)
    for j in range(per_row):
        lines[pl.ds(j, slots_all, stride=per_row), :] = picked[:, j * 128 : (j + 1) * 128]
    out_ref[...] = lines[...].astype(bf16)
    own_ref[...] = pick_part(lax.axis_index("tp"), after, own_ref.shape[1])


def expert_body(capacity, x_ref, gate_ref, up_ref, down_ref, out_ref, lines, sent):
    width = gate_ref.shape[1]
    per_row = width // 128
    count = x_ref.shape[0]
    sources = count // (capacity * per_row)
    lines[:count] = x_ref[...].astype(f32)
    lines[count:] = jnp.zeros((lines.shape[0] - count, 128), f32)
    x = jnp.concatenate(
        [
            jnp.concatenate(
                [
                    lines[pl.ds(e * capacity * per_row + j, 8, stride=per_row), :]
                    for j in range(per_row)
                ],
                axis=1,
            )
            for e in range(sources)
        ],
        axis=0,
    ).astype(bf16)
    hidden = (jax.nn.silu(dot(x, gate_ref[0])) * dot(x, up_ref[0])).astype(bf16)
    y = dot(hidden, down_ref[0])
    targets, chunk, _ = out_ref.shape
    tp_count = targets // sources
    per_part = per_row // tp_count
    for d in range(targets):
        e, t = d // tp_count, d % tp_count
        for j in range(per_part):
            lane = (t * per_part + j) * 128
            sent[pl.ds(d * chunk + j, 8, stride=per_part), :] = y[
                e * 8 : (e + 1) * 8, lane : lane + 128
            ]
    for d in range(targets):
        out_ref[d] = sent[d * chunk : (d + 1) * chunk].astype(bf16)


def combine_body(back_ref, ids_ref, weight_ref, own_ref, out_ref, lines):
    targets, chunk, _ = back_ref.shape
    tp_count = lax.axis_size("tp")
    experts = targets // tp_count
    per_part = own_ref.shape[1] // 128
    for d in range(targets):
        lines[d * chunk : (d + 1) * chunk] = back_ref[d].astype(f32)
    lines[targets * chunk :] = jnp.zeros((lines.shape[0] - targets * chunk, 128), f32)

    def piece(e, j):
        return sum(
            lines[pl.ds((e * tp_count + t) * chunk + j, 8, stride=per_part), :]
            for t in range(tp_count)
        )

    rows = jnp.concatenate(
        [
            jnp.concatenate([piece(e, j) for j in range(per_part)], axis=1)
            for e in range(experts)
        ],
        axis=0,
    ).astype(bf16)
    here, named = slots_of(ids_ref[...], 8, experts)
    weight = sum(jnp.where(n, weight_ref[k : k + 1], 0.0) for k, n in enumerate(named))
    weight = weight * here
    high = weight.astype(bf16)
    low = (weight - high.astype(f32)).astype(bf16)
    total = sum(
        lax.dot_general(w, rows, (((0,), (0,)), ((), ())), preferred_element_type=f32)
        for w in (high, low)
    )
    out_ref[...] = (own_ref[...] + total).astype(bf16)


def capacity_of(seqs, tops, experts):
    return max(2, seqs * tops // experts + 1)


def shards(
    residual_in,
    rec_state,
    mix_gain,
    w_query,
    w_forget,
    w_input,
    w_gate,
    lower_bound,
    head_gain,
    w_out,
    ffn_gain,
    route_ids,
    route_weight,
    expert_gate,
    expert_up,
    expert_down,
):
    deep, wide, cores, tp_count = (lax.axis_size(a) for a in ("a", "b", "c", "tp"))
    groups = deep * wide
    chips = ("a", "b")
    seqs, width = residual_in.shape
    part = width // tp_count
    cols = w_query.shape[1]
    _, heads, size, _ = rec_state.shape
    rows = up(seqs, 16)
    sds = jax.ShapeDtypeStruct

    sources = [residual_in, mix_gain]
    sources += [w.T for w in (w_query, w_forget, w_input, w_gate, w_out)]
    vmem, hbm = (pl.BlockSpec(memory_space=m) for m in (pltpu.VMEM, pltpu.HBM))
    spread, own_w, own_o = call(
        norm_body,
        [
            sds((groups, rows, part), bf16),
            sds((4, cols, part), bf16),
            sds((cols, part), bf16),
        ],
        *(pltpu.with_memory_space_constraint(a, pltpu.HBM) for a in sources),
        in_specs=[hbm] * 7,
        out_specs=[vmem] * 3,
        scratch_shapes=[
            pltpu.VMEM(residual_in.shape, bf16),
            pltpu.VMEM(mix_gain.shape, f32),
            pltpu.SemaphoreType.DMA((7,)),
        ],
    )
    swap = [(i, i ^ 1) for i in range(cores)]
    oth_w = lax.ppermute(own_w, "c", swap)
    if deep == 4:
        far = lax.ppermute(own_o, "a", [(i, i ^ 2) for i in range(deep)])
        side = lax.ppermute(own_o, "a", [(i, i ^ 1) for i in range(deep)])
    gathered = lax.all_to_all(spread, chips, 0, 0, tiled=True)

    partial = call(
        proj_body,
        sds((groups, tp_count, rows, 4 * cores * cols), bf16),
        gathered,
        own_w,
        oth_w,
    )
    if deep == 4:
        packs = [call(pack_body, sds((2, cols, part), bf16), own_o, far)]
        near = lax.ppermute(far, "a", [(i, i ^ 1) for i in range(deep)])
        packs.append(lax.ppermute(packs[0], "c", swap))
        packs += [side, lax.ppermute(side, "c", swap)]
        packs += [near, lax.ppermute(near, "c", swap)]
    else:
        packs = [lax.all_gather(own_o, ("a", "c"), axis=0).reshape(-1, part)]
    arrived = lax.all_to_all(
        partial.reshape(groups * tp_count, rows, -1), (*chips, "tp"), 0, 0, tiled=True
    ).reshape(partial.shape)

    own_heads, forget, value = call(
        read_body,
        [
            sds((rows, heads * size), bf16),
            sds((rows, heads * size), f32),
            sds((rows, heads * size), f32),
        ],
        arrived,
        lower_bound,
        head_gain,
        rec_state,
    )
    all_heads = [own_heads] + [
        lax.ppermute(own_heads, "b", [(i, (i + s) % wide) for i in range(wide)])
        for s in range(1, wide)
    ]

    per_head = pl.BlockSpec((seqs, 1, size, size), lambda i: (0, i, 0, 0))
    head_lanes = pl.BlockSpec((rows, size), lambda i: (0, i))
    new_state = call(
        state_body,
        sds(rec_state.shape, bf16),
        forget,
        value,
        rec_state,
        grid=(heads,),
        in_specs=[head_lanes, head_lanes, per_head],
        out_specs=per_head,
        cost=pl.CostEstimate(
            flops=10**7, bytes_accessed=4 * rec_state.size, transcendentals=0
        ),
    )

    partial_mix = call(
        functools.partial(mix_body, wide),
        [sds((rows, deep * cores * cols), bf16)] * wide,
        *all_heads,
        *packs,
    )
    mix_home = []
    for i in range(wide):
        for t in range(tp_count):
            perm = [
                (b * tp_count + p, (b + i) % wide * tp_count + (p + t) % tp_count)
                for b in range(wide)
                for p in range(tp_count)
            ]
            moved = lax.ppermute(partial_mix[i], ("b", "tp"), perm) if i + t else partial_mix[0]
            mix_home.append(moved)

    experts = groups * cores
    capacity = capacity_of(seqs, route_ids.shape[1], experts)
    assert capacity <= 8
    lines = experts * capacity * width // 128
    buffer, own_mix = call(
        functools.partial(dispatch_body, wide),
        [sds((lines, 128), bf16), sds((seqs, part), f32)],
        *mix_home,
        residual_in,
        ffn_gain,
        route_ids.T,
        scratch_shapes=[pltpu.VMEM((lines, 128), f32)],
    )
    received = lax.all_to_all(
        buffer.reshape(experts, -1, 128), (*chips, "c"), 0, 0, tiled=True
    ).reshape(lines, 128)
    per_part = part // 128
    chunk = up(capacity * per_part, 8)
    targets = experts * tp_count
    sent = targets * chunk + 8 * per_part
    down = call(
        functools.partial(expert_body, capacity),
        sds((targets, chunk, 128), bf16),
        received,
        expert_gate,
        expert_up,
        expert_down,
        scratch_shapes=[
            pltpu.VMEM((lines + 8 * width // 128, 128), f32),
            pltpu.VMEM((sent, 128), f32),
        ],
    )
    back = lax.all_to_all(down, (*chips, "c", "tp"), 0, 0, tiled=True)
    layer_out = call(
        combine_body,
        sds((seqs, part), bf16),
        back,
        route_ids.T,
        route_weight.T,
        own_mix,
        scratch_shapes=[pltpu.VMEM((sent, 128), f32)],
    )
    return layer_out, new_state


def solution(mesh):
    ep, tp = mesh.shape["ep"], mesh.shape["tp"]
    wide = 2 if ep % 4 == 0 else 1
    shape = (ep // (2 * wide), wide, 2, tp)
    split = Mesh(mesh.devices.reshape(shape), ("a", "b", "c", "tp"))
    seq = ("a", "b", "c")
    in_specs = (
        P(seq, None),
        P(seq, "tp", None, None),
        P(),
        P("tp", seq),
        P("tp", seq),
        P("tp", seq),
        P("tp", seq),
        P("tp"),
        P(),
        P("tp", seq),
        P(),
        P(seq, None),
        P(seq, None),
        P(seq, None, "tp"),
        P(seq, None, "tp"),
        P(seq, "tp", None),
    )
    out_specs = (P(seq, "tp"), P(seq, "tp", None, None))
    return jax.shard_map(
        shards, mesh=split, in_specs=in_specs, out_specs=out_specs, check_vma=False
    )
```
